256 devices in a mesh: st: 32 (over z, x), tp: 8 (over y, core).
Axes of the slice: x: 4, y: 4, z: 8, core: 2. Of those that a mesh axis runs over, the one named last changes fastest.
Arguments:
- symbol_activations: bfloat16 [24576, 2048], P('st', 'tp'), may hold values from -6 to 6
- document_corpus: bfloat16 [512, 96, 2048], P('st'), may hold values from -6 to 6
- document_choice_matrix: int32 [192, 4], P('st'), may hold values from 0 to 511, as said below
- memory_probe_matrix: bfloat16 [2048, 1024], P(None, 'tp'), may hold values from -0.125 to 0.125
- memory_lookup_matrix: bfloat16 [2048, 1024], P(None, 'tp'), may hold values from -0.125 to 0.125
- memory_content_matrix: bfloat16 [2048, 1024], P(None, 'tp'), may hold values from -0.125 to 0.125
- valve_matrix: bfloat16 [2048, 16], replicated, may hold values from -0.125 to 0.125
- valve_biases: float32 [16], replicated, may hold values from -3 to 9
- added_decay_logit: float32 [24576, 8], P('st'), may hold values from -1 to 0
- facet_rescale_factor: float32 [1024], P('tp'), may hold values from 0.1 to 1.9
- document_probe_matrix: bfloat16 [2048, 1024], P(None, 'tp'), may hold values from -0.125 to 0.125
- document_lookup_matrix: bfloat16 [2048, 1024], P(None, 'tp'), may hold values from -0.125 to 0.125
- document_content_matrix: bfloat16 [2048, 1024], P(None, 'tp'), may hold values from -0.125 to 0.125
- document_rescale_factor: float32 [2048], replicated, may hold values from 0.1 to 1.9
- affinity_scaling: float32 [8], replicated, may hold values from 8 to 1200
- fetched_mixer_matrix: bfloat16 [2048, 1024], P(None, 'tp'), may hold values from -0.125 to 0.125
Outputs:
- mixed: bfloat16 [24576, 1024], P('st', 'tp')
The draws below stay inside these ranges and needn't reach their ends.
Inputs may be any that keep to these rules, and one draw needn't show every extreme that they name: `document_choice_matrix`: row b names the 4 passages that block b reads; passage p is held by index p // 16 of st. Among the rows of one sequence at most 2 ids name passages of one holder, and some holder is named exactly 2 times by each sequence.
All inputs are finite; a program needn't handle non-finite values.
Results may differ from the reference program's by a relative error of at most 0.0095.
The reference program's roundings to bfloat16 on the way count: a program that leaves them out, or rounds other values in their place, can miss the bound.
Values may be sent and summed in bfloat16 or wider, within the bound.
No kernel may reach another device: no remote copies, remote signals or barrier semaphores. Data moves between devices by JAX's collectives and lax.ppermute only.
A program may use at most 128 MiB of HBM per device.

```python
import jax
import jax.numpy as jnp
from jax import lax

MODEL_WIDTH = 2048
FACET_COUNT = 8
LANE_DIMENSION = 128
STRING_LENGTH = 768
BLK = 128
SEG = 128
PASSAGE_READS = 4
PLEN = 96
P_DEV = 16
TOKENS = 24576
SEQUENCE_BLOCKS = 6
PASSAGES = 512
N_ST = 32


def draw_document_choice_matrix(key, part):
    request_count = STRING_LENGTH // BLK * PASSAGE_READS
    slot_cap = max(2, 2 * request_count // N_ST)
    slot_total = N_ST * slot_cap
    popular_key, device_key = jax.random.split(jax.random.fold_in(key, 11))
    popular = jax.random.randint(popular_key, (N_ST,), 0, 4)
    owner_of = jnp.arange(slot_total, dtype=jnp.int32) // slot_cap
    rank_in = jnp.arange(slot_total, dtype=jnp.int32) % slot_cap

    def one_device(device):
        sub_key = jax.random.fold_in(device_key, device)
        noise_key, shuffle_key, first_key, second_key = jax.random.split(sub_key, 4)
        score = jax.random.randint(noise_key, (slot_total,), 0, 65536) - popular[owner_of] * 65536
        before = (device + N_ST - 1) % N_ST
        across = (device + N_ST // 2) % N_ST
        score = jnp.where(owner_of == before, -(1 << 30), score)
        score = jnp.where((owner_of == across) & (rank_in == 0), -(1 << 29), score)
        chosen = jnp.argsort(score, stable=True)[:request_count]
        owners = owner_of[chosen][jax.random.permutation(shuffle_key, request_count)]
        within = jnp.minimum(jax.random.randint(first_key, (request_count,), 0, P_DEV), jax.random.randint(second_key, (request_count,), 0, P_DEV))
        return (owners * P_DEV + within).astype(jnp.int32)
    picked = jax.vmap(one_device)(jnp.arange(N_ST, dtype=jnp.int32))
    return picked.reshape(N_ST * request_count // PASSAGE_READS, PASSAGE_READS)


def draw_valve_biases(key, part):
    input_key, pick_key, noise_key = jax.random.split(jax.random.fold_in(key, 23), 3)
    input_rows = 0.5 * jax.random.normal(input_key, (FACET_COUNT,), jnp.float32)
    slow = jnp.log(jnp.float32(STRING_LENGTH))
    fast = jnp.log(jnp.float32(40.0))
    pick = jax.random.bernoulli(pick_key, 0.5, (FACET_COUNT,))
    forget = jnp.where(pick, slow, fast) + 0.3 * jax.random.normal(noise_key, (FACET_COUNT,), jnp.float32)
    return jnp.clip(jnp.concatenate([input_rows, forget]), -3.0, 9.0).astype(jnp.float32)


def draw_added_decay_logit(key, part):
    mask_key, depth_key = jax.random.split(jax.random.fold_in(key, 37))
    marked = jax.random.bernoulli(mask_key, 3.0 / STRING_LENGTH, (TOKENS, FACET_COUNT))
    depth = jnp.log(jax.random.uniform(depth_key, (TOKENS, FACET_COUNT), jnp.float32, 0.5, 0.8))
    return jnp.where(marked, depth, 0.0).astype(jnp.float32)


def draw_affinity_scaling(key, part):
    sub_key = jax.random.fold_in(key, 41)
    spread = jax.random.uniform(sub_key, (FACET_COUNT,), jnp.float32, jnp.log(8.0), jnp.log(24.0))
    return jnp.exp(spread).astype(jnp.float32)


def level_of(rng, extent, cuts, least, largest):
    factor_of, own = 1.0, jax.random.fold_in(rng, 6)
    for position, shards_of in cuts:
        draws = jnp.exp(jax.random.uniform(jax.random.fold_in(own, position), (shards_of,), jnp.float32, least / len(cuts), largest / len(cuts)))
        factor_of = factor_of * jnp.repeat(draws, extent[position] // shards_of).reshape([-1 if axis == position else 1 for axis in range(len(extent))])
    return factor_of


def centred(stream_key, dims, deviation, bound, pieces=(), kind=jnp.bfloat16):
    factor_of = level_of(stream_key, dims, pieces, -0.22, 0.18) if pieces else 1.0
    array = jax.random.normal(stream_key, dims, jnp.float32) * deviation * factor_of
    return jnp.minimum(jnp.maximum(array, -bound), bound).astype(kind)


def setup_inputs(seed: int = 0) -> dict:
    splits = jax.random.split(jax.random.key(seed), 17)
    symbol_activations = centred(splits[0], (TOKENS, MODEL_WIDTH), 1.0, 6.0, ((0, 32), (1, 8)))
    document_corpus = centred(splits[1], (PASSAGES, PLEN, MODEL_WIDTH), 1.0, 6.0, ((0, 32),))
    document_choice_matrix = draw_document_choice_matrix(jax.random.fold_in(splits[16], 71), 0)
    memory_probe_matrix = centred(splits[3], (MODEL_WIDTH, FACET_COUNT * LANE_DIMENSION), MODEL_WIDTH ** -0.5, 0.125, ((1, 8),))
    memory_lookup_matrix = centred(splits[4], (MODEL_WIDTH, FACET_COUNT * LANE_DIMENSION), MODEL_WIDTH ** -0.5, 0.125, ((1, 8),))
    memory_content_matrix = centred(splits[5], (MODEL_WIDTH, FACET_COUNT * LANE_DIMENSION), MODEL_WIDTH ** -0.5, 0.125, ((1, 8),))
    valve_matrix = centred(splits[6], (MODEL_WIDTH, 2 * FACET_COUNT), MODEL_WIDTH ** -0.5, 0.125)
    valve_biases = draw_valve_biases(jax.random.fold_in(splits[16], 71), 0)
    added_decay_logit = draw_added_decay_logit(jax.random.fold_in(splits[16], 71), 0)
    facet_rescale_factor = jnp.clip(1.0 + 0.18 * jax.random.normal(splits[9], (FACET_COUNT * LANE_DIMENSION,), jnp.float32), 0.1, 1.9)
    document_probe_matrix = centred(splits[10], (MODEL_WIDTH, FACET_COUNT * LANE_DIMENSION), MODEL_WIDTH ** -0.5, 0.125, ((1, 8),))
    document_lookup_matrix = centred(splits[11], (MODEL_WIDTH, FACET_COUNT * LANE_DIMENSION), MODEL_WIDTH ** -0.5, 0.125, ((1, 8),))
    document_content_matrix = centred(splits[12], (MODEL_WIDTH, FACET_COUNT * LANE_DIMENSION), MODEL_WIDTH ** -0.5, 0.125, ((1, 8),))
    document_rescale_factor = jnp.clip(1.0 + 0.18 * jax.random.normal(splits[13], (MODEL_WIDTH,), jnp.float32), 0.1, 1.9)
    affinity_scaling = draw_affinity_scaling(jax.random.fold_in(splits[16], 71), 0)
    fetched_mixer_matrix = centred(splits[15], (MODEL_WIDTH, FACET_COUNT * LANE_DIMENSION), MODEL_WIDTH ** -0.5, 0.125, ((1, 8),))
    return dict(symbol_activations=symbol_activations, document_corpus=document_corpus, document_choice_matrix=document_choice_matrix, memory_probe_matrix=memory_probe_matrix, memory_lookup_matrix=memory_lookup_matrix, memory_content_matrix=memory_content_matrix, valve_matrix=valve_matrix, valve_biases=valve_biases, added_decay_logit=added_decay_logit, facet_rescale_factor=facet_rescale_factor, document_probe_matrix=document_probe_matrix, document_lookup_matrix=document_lookup_matrix, document_content_matrix=document_content_matrix, document_rescale_factor=document_rescale_factor, affinity_scaling=affinity_scaling, fetched_mixer_matrix=fetched_mixer_matrix)


EPSILON = 1e-06
EMPTY_LOG = -1e+30
HIGHEST = lax.Precision.HIGHEST

def rms_scale(tensor):
    return lax.rsqrt(lax.optimization_barrier(jnp.mean(tensor * tensor, axis=-1, keepdims=True)) + EPSILON)

def cell_blocks(queries, key_rows, value_rows, input_logits, forget_log_gate):
    head_count, length, facet_dimension = queries.shape
    block_count = length // SEG

    def to_blocks(tensor):
        shaped = tensor.reshape((head_count, block_count, SEG) + tensor.shape[2:])
        return jnp.moveaxis(shaped, 1, 0)
    causal = jnp.tril(jnp.ones((SEG, SEG), dtype=bool))

    def advance(carry, blocks):
        memory, normal, stabilizer = carry
        query_part, key_part, value_part, input_part, forget_part = blocks
        cumulative = jnp.cumsum(forget_part, axis=-1)
        log_weight = jnp.where(causal, cumulative[:, :, None] - cumulative[:, None, :] + input_part[:, None, :], -jnp.inf)
        carried = cumulative + stabilizer[:, None]
        peak = jnp.maximum(carried, lax.optimization_barrier(jnp.max(log_weight, axis=-1)))
        weight = jnp.exp(log_weight - peak[:, :, None])
        old_weight = jnp.exp(carried - peak)
        affinity_logits = jnp.einsum('htd,hsd->hts', query_part, key_part, precision=HIGHEST) * weight
        numerator = old_weight[:, :, None] * jnp.einsum('htd,hde->hte', query_part, memory, precision=HIGHEST) + jnp.einsum('hts,hse->hte', affinity_logits, value_part, precision=HIGHEST)
        denominator = old_weight * jnp.einsum('htd,hd->ht', query_part, normal, precision=HIGHEST) + lax.optimization_barrier(jnp.sum(affinity_logits, axis=-1))
        final_output = numerator / jnp.maximum(jnp.abs(denominator), jnp.exp(-peak))[:, :, None]
        last_weight = weight[:, -1, :]
        old_last = old_weight[:, -1]
        weighted_keys = last_weight[:, :, None] * key_part
        memory = old_last[:, None, None] * memory + jnp.einsum('hsd,hse->hde', weighted_keys, value_part, precision=HIGHEST)
        normal = old_last[:, None] * normal + lax.optimization_barrier(jnp.sum(weighted_keys, axis=1))
        return ((memory, normal, peak[:, -1]), final_output)
    initial = (jnp.zeros((head_count, facet_dimension, facet_dimension), jnp.float32), jnp.zeros((head_count, facet_dimension), jnp.float32), jnp.full((head_count,), EMPTY_LOG, jnp.float32))
    scaled_keys = key_rows * facet_dimension ** (-0.5)
    final_state, outcome = lax.scan(advance, initial, (to_blocks(queries), to_blocks(scaled_keys), to_blocks(value_rows), to_blocks(input_logits), to_blocks(forget_log_gate)))
    return jnp.moveaxis(outcome, 0, 1).reshape(head_count, length, facet_dimension)

def document_lookup_update(probe_vectors, segment_lookups, segment_contents, facet_scales):
    facet_dimension = probe_vectors.shape[-1]
    affinity_logits = jnp.einsum('bqhd,bkhd->bhqk', probe_vectors.astype(jnp.float32), segment_lookups.astype(jnp.float32))
    ask_scale = rms_scale(probe_vectors.astype(jnp.float32))[..., 0]
    key_scale = rms_scale(segment_lookups.astype(jnp.float32))[..., 0]
    affinity_logits = affinity_logits * jnp.transpose(ask_scale, (0, 2, 1))[:, :, :, None]
    affinity_logits = affinity_logits * jnp.transpose(key_scale, (0, 2, 1))[:, :, None, :]
    affinity_logits = affinity_logits * (facet_scales / facet_dimension)[None, :, None, None]
    peak = lax.optimization_barrier(jnp.max(affinity_logits, axis=-1, keepdims=True))
    exp_scores = jnp.exp(affinity_logits - peak)
    weights = (exp_scores / lax.optimization_barrier(jnp.sum(exp_scores, axis=-1, keepdims=True))).astype(jnp.bfloat16)
    return jnp.einsum('bhqk,bkhd->bqhd', weights.astype(jnp.float32), segment_contents.astype(jnp.float32))

def reference(symbol_activations, document_corpus, document_choice_matrix, memory_probe_matrix, memory_lookup_matrix, memory_content_matrix, valve_matrix, valve_biases, added_decay_logit, facet_rescale_factor, document_probe_matrix, document_lookup_matrix, document_content_matrix, document_rescale_factor, affinity_scaling, fetched_mixer_matrix):
    store_rows = document_corpus.reshape(PASSAGES * PLEN, MODEL_WIDTH).astype(jnp.float32)
    normed = (store_rows * rms_scale(store_rows) * document_rescale_factor).astype(jnp.bfloat16)
    store_keys = jnp.dot(normed, document_lookup_matrix, preferred_element_type=jnp.float32).astype(jnp.bfloat16).reshape(PASSAGES, PLEN, FACET_COUNT * LANE_DIMENSION)
    store_values = jnp.dot(normed, document_content_matrix, preferred_element_type=jnp.float32).astype(jnp.bfloat16).reshape(PASSAGES, PLEN, FACET_COUNT * LANE_DIMENSION)

    def single_sequence(input_rows):
        sequence_token_rows, sequence_passage_index, sequence_extra_forget = input_rows

        def project(weight):
            return jnp.dot(sequence_token_rows, weight, preferred_element_type=jnp.float32)

        def heads_first(tensor):
            return jnp.transpose(tensor.astype(jnp.float32).reshape(STRING_LENGTH, FACET_COUNT, LANE_DIMENSION), (1, 0, 2))
        queries = project(memory_probe_matrix).astype(jnp.bfloat16)
        key_rows = project(memory_lookup_matrix).astype(jnp.bfloat16)
        value_rows = project(memory_content_matrix).astype(jnp.bfloat16)
        probe_vectors = project(document_probe_matrix).astype(jnp.bfloat16)
        mix_logits = project(fetched_mixer_matrix)
        gate_preactivation = project(valve_matrix) + valve_biases
        input_logits = gate_preactivation[:, :FACET_COUNT]
        forget_log_gate = jax.nn.log_sigmoid(gate_preactivation[:, FACET_COUNT:]) + sequence_extra_forget
        cell_out = cell_blocks(heads_first(queries), heads_first(key_rows), heads_first(value_rows), input_logits.T, forget_log_gate.T)
        cell_out = cell_out * rms_scale(cell_out) * facet_rescale_factor.reshape(FACET_COUNT, 1, LANE_DIMENSION)
        cell_out = jnp.transpose(cell_out, (1, 0, 2)).reshape(STRING_LENGTH, FACET_COUNT * LANE_DIMENSION)
        segment_lookups = store_keys[sequence_passage_index].reshape(SEQUENCE_BLOCKS, PASSAGE_READS * PLEN, FACET_COUNT, LANE_DIMENSION)
        segment_contents = store_values[sequence_passage_index].reshape(SEQUENCE_BLOCKS, PASSAGE_READS * PLEN, FACET_COUNT, LANE_DIMENSION)
        segment_probes = probe_vectors.reshape(SEQUENCE_BLOCKS, STRING_LENGTH // SEQUENCE_BLOCKS, FACET_COUNT, LANE_DIMENSION)
        fetched_result = document_lookup_update(segment_probes, segment_lookups, segment_contents, affinity_scaling).reshape(STRING_LENGTH, FACET_COUNT * LANE_DIMENSION)
        return (cell_out + jax.nn.sigmoid(mix_logits) * fetched_result).astype(jnp.bfloat16)
    final_output = lax.map(single_sequence, (symbol_activations.reshape(N_ST, STRING_LENGTH, MODEL_WIDTH), document_choice_matrix.reshape(N_ST, SEQUENCE_BLOCKS, PASSAGE_READS), added_decay_logit.reshape(N_ST, STRING_LENGTH, FACET_COUNT)))
    return final_output.reshape(TOKENS, FACET_COUNT * LANE_DIMENSION)
```

```python
import functools

import jax
import jax.numpy as jnp
from jax import lax
from jax.experimental import pallas as pl
from jax.experimental.pallas import tpu as pltpu
from jax.sharding import PartitionSpec as P

FACETS = 8
LANES = 128
SEG = 128
EPS = 1e-06
EMPTY_LOG = -1e30
NZ = 8
NX = 4
F32 = jnp.float32
BF16 = jnp.bfloat16


def dot(a, b, dims=((1,), (0,))):
    return lax.dot_general(a, b, (dims, ((), ())), preferred_element_type=F32)


def split_bf16(a):
    high = a.astype(BF16)
    return high, (a - high.astype(F32)).astype(BF16)


def passage_kernel(rows_ref, gain_ref, wk_ref, wv_ref, k_ref, v_ref, w_scr, n_scr):
    @pl.when(pl.program_id(0) == 0)
    def _():
        w_scr[:, :LANES] = wk_ref[...]
        w_scr[:, LANES:] = wv_ref[...]

    count, length, width = rows_ref.shape
    step = 16
    for p in range(count):
        for r in range(0, length, step):
            x = rows_ref[p, r : r + step, :].astype(F32)
            scale = lax.rsqrt(jnp.sum(x * x, axis=-1, keepdims=True) / width + EPS)
            n_scr[p * length + r : p * length + r + step, :] = (
                x * scale * gain_ref[...]
            ).astype(BF16)
    both = dot(n_scr[...], w_scr[...]).astype(BF16)
    k_ref[...] = both[:, :LANES].reshape(count, length, LANES)
    v_ref[...] = both[:, LANES:].reshape(count, length, LANES)


def passage_projection(corpus, gain, wk, wv):
    count, length, width = corpus.shape
    per = 4
    out = jax.ShapeDtypeStruct((count, length, LANES), BF16)
    return pl.pallas_call(
        passage_kernel,
        grid=(count // per,),
        in_specs=[
            pl.BlockSpec((per, length, width), lambda i: (i, 0, 0)),
            pl.BlockSpec((1, width), lambda i: (0, 0)),
            pl.BlockSpec((width, LANES), lambda i: (0, 0)),
            pl.BlockSpec((width, LANES), lambda i: (0, 0)),
        ],
        out_specs=[pl.BlockSpec((per, length, LANES), lambda i: (i, 0, 0))] * 2,
        out_shape=[out, out],
        scratch_shapes=[
            pltpu.VMEM((width, 2 * LANES), BF16),
            pltpu.VMEM((per * length, width), BF16),
        ],
        name="passage_projection",
    )(corpus, gain.reshape(1, width), wk, wv)


def token_kernel(head_ref, *refs):
    pieces = refs[:8]
    weights = refs[8:13]
    valve_ref, bias_ref, decay_ref = refs[13:16]
    q_ref, k_ref, v_ref, ask_ref, mix_ref, gate_ref = refs[16:22]
    h_scr, w_scr, sems = refs[22:]
    copies = []
    for i, w in enumerate(weights):
        copies.append(
            pltpu.make_async_copy(w, w_scr.at[:, i * LANES : (i + 1) * LANES], sems.at[i])
        )
    width = pieces[0].shape[1]
    for i, piece in enumerate(pieces):
        start = pl.multiple_of(head_ref[1 + i] * width, width)
        copies.append(
            pltpu.make_async_copy(piece, h_scr.at[:, pl.ds(start, width)], sems.at[5 + i])
        )
    for c in copies:
        c.start()
    valve = valve_ref[...]
    w_scr[:, 5 * LANES :] = jnp.concatenate(
        [valve, jnp.zeros((valve.shape[0], LANES - valve.shape[1]), BF16)], axis=1
    )
    for c in copies:
        c.wait()
    h = h_scr[...]
    qk = dot(h, w_scr[:, : 2 * LANES]).astype(BF16)
    q_ref[...] = qk[:, :LANES]
    k_ref[...] = qk[:, LANES:]
    va = dot(h, w_scr[:, 2 * LANES : 4 * LANES]).astype(BF16)
    v_ref[...] = va[:, :LANES]
    ask_ref[...] = va[:, LANES:]
    mg = dot(h, w_scr[:, 4 * LANES :])
    mix_ref[...] = mg[:, :LANES]
    head = head_ref[0]
    lane = lax.broadcasted_iota(jnp.int32, (h.shape[0], LANES), 1)
    gates = mg[:, LANES:] + bias_ref[...]
    decay_lane = lax.broadcasted_iota(jnp.int32, decay_ref.shape, 1)

    def pick(array, lanes, which):
        return jnp.sum(jnp.where(lanes == which, array, 0.0), axis=1, keepdims=True)

    incoming = pick(gates, lane, head)
    forget = pick(gates, lane, FACETS + head)
    log_forget = (
        jnp.minimum(forget, 0.0)
        - jnp.log1p(jnp.exp(-jnp.abs(forget)))
        + pick(decay_ref[...], decay_lane, head)
    )
    gate_ref[...] = jnp.where(lane == 0, incoming, log_forget)


def token_projection(order, pieces, weights, valve, bias, decay):
    rows = pieces[0].shape[0]
    width = valve.shape[0]
    half = jax.ShapeDtypeStruct((rows, LANES), BF16)
    full = jax.ShapeDtypeStruct((rows, LANES), F32)
    vmem = pl.BlockSpec(memory_space=pltpu.VMEM)
    hbm = pl.BlockSpec(memory_space=pl.ANY)
    padded = jnp.pad(bias, (0, LANES - bias.shape[0])).reshape(1, LANES)
    return pl.pallas_call(
        token_kernel,
        in_specs=[pl.BlockSpec(memory_space=pltpu.SMEM)] + [hbm] * 13 + [vmem] * 3,
        out_specs=[vmem] * 6,
        out_shape=[half] * 4 + [full] * 2,
        scratch_shapes=[
            pltpu.VMEM((rows, width), BF16),
            pltpu.VMEM((width, 6 * LANES), BF16),
            pltpu.SemaphoreType.DMA((13,)),
        ],
        name="token_projection",
    )(order, *pieces, *weights, valve, padded, decay)


def cell_kernel(q_ref, k_ref, v_ref, gate_ref, facet_ref, out_ref):
    row = lax.broadcasted_iota(jnp.int32, (SEG, SEG), 0)
    col = lax.broadcasted_iota(jnp.int32, (SEG, SEG), 1)
    causal = row >= col
    eye = row == col
    scale = LANES ** (-0.5)

    def to_row(column):
        return jnp.sum(jnp.where(eye, column, 0.0), axis=0, keepdims=True)

    memory = jnp.zeros((LANES, LANES), F32)
    normal = jnp.zeros((1, LANES), F32)
    stabilizer = jnp.full((1, 1), EMPTY_LOG, F32)
    for b in range(q_ref.shape[0] // SEG):
        part = slice(b * SEG, (b + 1) * SEG)
        q = q_ref[part, :]
        k = k_ref[part, :]
        v = v_ref[part, :]
        in_col = gate_ref[part, 0:1]
        forget_col = gate_ref[part, 1:2]
        cum_col = jnp.sum(jnp.where(causal, to_row(forget_col), 0.0), axis=1, keepdims=True)
        source = to_row(in_col - cum_col)
        log_weight = jnp.where(causal, cum_col + source, -jnp.inf)
        carried = cum_col + stabilizer
        peak = jnp.maximum(carried, jnp.max(log_weight, axis=1, keepdims=True))
        weight = jnp.exp(log_weight - peak)
        old = jnp.exp(carried - peak)
        logits = dot(q, k, ((1,), (1,))) * scale * weight
        high, low = split_bf16(logits)
        mem_high, mem_low = split_bf16(memory)
        numerator = old * (dot(q, mem_high) + dot(q, mem_low)) + (dot(high, v) + dot(low, v))
        denominator = old * jnp.sum(q.astype(F32) * normal, axis=1, keepdims=True) + jnp.sum(
            logits, axis=1, keepdims=True
        )
        cell = numerator / jnp.maximum(jnp.abs(denominator), jnp.exp(-peak))
        square = jnp.mean(cell * cell, axis=1, keepdims=True)
        out_ref[part, :] = cell * lax.rsqrt(square + EPS) * facet_ref[...]
        peak_last = peak[SEG - 1 :, :]
        cum_last = cum_col[SEG - 1 :, :]
        old_last = old[SEG - 1 :, :]
        last = jnp.exp(cum_last - cum_col + in_col - peak_last)
        weighted = k.astype(F32) * scale * last
        wk_high, wk_low = split_bf16(weighted)
        memory = old_last * memory + (
            dot(wk_high, v, ((0,), (0,))) + dot(wk_low, v, ((0,), (0,)))
        )
        normal = old_last * normal + jnp.sum(weighted, axis=0, keepdims=True)
        stabilizer = peak_last


def cell_block(q, k, v, gates, facet):
    vmem = pl.BlockSpec(memory_space=pltpu.VMEM)
    return pl.pallas_call(
        cell_kernel,
        in_specs=[vmem] * 5,
        out_specs=vmem,
        out_shape=jax.ShapeDtypeStruct(q.shape, F32),
        name="cell",
    )(q, k, v, gates, facet.reshape(1, LANES))


def select_kernel(deltas, index_ref, *refs):
    arrays = refs[: 2 * len(deltas)]
    out_ref, sems = refs[2 * len(deltas) :]
    copies = []
    for p, delta in enumerate(deltas):
        for reader in range(NX):
            for slot in range(2):
                at = index_ref[(delta * NX + reader) * 2 + slot]
                for kind in range(2):
                    copies.append(
                        pltpu.make_async_copy(
                            arrays[2 * p + kind].at[at],
                            out_ref.at[reader, p, slot, kind],
                            sems.at[len(copies)],
                        )
                    )
    for c in copies:
        c.start()
    for c in copies:
        c.wait()


def select(index, planes):
    deltas = [d for d, _, _ in planes]
    arrays = [a for _, k, v in planes for a in (k, v)]
    hbm = pl.BlockSpec(memory_space=pl.ANY)
    _, length, lanes = arrays[0].shape
    return pl.pallas_call(
        functools.partial(select_kernel, deltas),
        in_specs=[pl.BlockSpec(memory_space=pltpu.SMEM)] + [hbm] * len(arrays),
        out_specs=hbm,
        out_shape=jax.ShapeDtypeStruct((NX, len(deltas), 2, 2, length, lanes), BF16),
        scratch_shapes=[pltpu.SemaphoreType.DMA((len(deltas) * NX * 4,))],
        name="select",
    )(index, *arrays)


def read_kernel(groups, place_ref, scale_ref, *refs):
    stages = refs[: len(groups)]
    ask_ref, mix_ref, cell_ref, out_ref, kv_scr, k_scr, v_scr, sems = refs[len(groups) :]
    copies = []
    for stage, deltas in zip(stages, groups):
        for p, delta in enumerate(deltas):
            copies.append(
                pltpu.make_async_copy(stage.at[:, p], kv_scr.at[delta], sems.at[len(copies)])
            )
    for c in copies:
        c.start()
    for c in copies:
        c.wait()
    row = lax.broadcasted_iota(jnp.int32, (SEG, SEG), 0)
    col = lax.broadcasted_iota(jnp.int32, (SEG, SEG), 1)
    eye = row == col
    length = k_scr.shape[0] // 4
    score_scale = scale_ref[0] / LANES
    for b in range(out_ref.shape[0] // SEG):
        part = slice(b * SEG, (b + 1) * SEG)
        for i in range(4):
            place = place_ref[b * 4 + i]
            delta = place // 8
            holder = (place // 2) % 4
            slot = place % 2
            rows = slice(i * length, (i + 1) * length)
            k_scr[rows, :] = kv_scr[delta, holder, slot, 0]
            v_scr[rows, :] = kv_scr[delta, holder, slot, 1]
        ask = ask_ref[part, :]
        keys = k_scr[...]
        ask32 = ask.astype(F32)
        key32 = keys.astype(F32)
        ask_scale = lax.rsqrt(jnp.mean(ask32 * ask32, axis=1, keepdims=True) + EPS)
        ask_row = jnp.sum(jnp.where(eye, ask_scale, 0.0), axis=0, keepdims=True)
        key_scale = lax.rsqrt(jnp.mean(key32 * key32, axis=1, keepdims=True) + EPS)
        scores = dot(keys, ask, ((1,), (1,))) * ask_row * key_scale * score_scale
        peak = jnp.max(scores, axis=0, keepdims=True)
        terms = jnp.exp(scores - peak)
        weights = (terms / jnp.sum(terms, axis=0, keepdims=True)).astype(BF16)
        retrieved = dot(weights, v_scr[...], ((0,), (0,)))
        gate = 1.0 / (1.0 + jnp.exp(-mix_ref[part, :]))
        out_ref[part, :] = (cell_ref[part, :] + gate * retrieved).astype(BF16)


def read_passages(place, scale, stages, ask, mix, cell):
    groups = [d for d, _ in stages]
    arrays = [a for _, a in stages]
    length, lanes = arrays[0].shape[-2:]
    vmem = pl.BlockSpec(memory_space=pltpu.VMEM)
    smem = pl.BlockSpec(memory_space=pltpu.SMEM)
    hbm = pl.BlockSpec(memory_space=pl.ANY)
    return pl.pallas_call(
        functools.partial(read_kernel, groups),
        in_specs=[smem, smem] + [hbm] * len(arrays) + [vmem] * 3,
        out_specs=vmem,
        out_shape=jax.ShapeDtypeStruct(ask.shape, BF16),
        scratch_shapes=[
            pltpu.VMEM((NZ, NX, 2, 2, length, lanes), BF16),
            pltpu.VMEM((4 * length, lanes), BF16),
            pltpu.VMEM((4 * length, lanes), BF16),
            pltpu.SemaphoreType.DMA((NZ,)),
        ],
        name="read_passages",
    )(place, scale, *arrays, ask, mix, cell)


def along_z(tensor, step):
    pairs = [(z * NX + x, (z + step) % NZ * NX + x) for z in range(NZ) for x in range(NX)]
    return lax.ppermute(tensor, "st", pairs)


def along_x(tensor):
    groups = [[z * NX + x for x in range(NX)] for z in range(NZ)]
    return lax.all_to_all(
        tensor, "st", split_axis=0, concat_axis=0, axis_index_groups=groups, tiled=True
    )


def to_tp(tensor, step, other):
    pairs = [
        (y * 2 + c, (y + step) % 4 * 2 + (1 - c if other else c)) for y in range(4) for c in range(2)
    ]
    return lax.ppermute(tensor, "tp", pairs)


def gather_tokens(tokens, rank):
    own = [tokens, to_tp(tokens, 1, False), to_tp(tokens, -1, False), to_tp(tokens, 2, False)]
    pieces = own + [to_tp(p, 0, True) for p in own]
    y, c = rank // 2, rank % 2
    ys = [y, (y + 3) % 4, (y + 1) % 4, (y + 2) % 4]
    order = [v * 2 + c for v in ys] + [v * 2 + 1 - c for v in ys]
    return pieces, jnp.stack([rank] + order).astype(jnp.int32)


def local(
    symbol_activations,
    document_corpus,
    document_choice_matrix,
    memory_probe_matrix,
    memory_lookup_matrix,
    memory_content_matrix,
    valve_matrix,
    valve_biases,
    added_decay_logit,
    facet_rescale_factor,
    document_probe_matrix,
    document_lookup_matrix,
    document_content_matrix,
    document_rescale_factor,
    affinity_scaling,
    fetched_mixer_matrix,
):
    rank = lax.axis_index("tp")
    st = lax.axis_index("st")
    z, x = st // NX, st % NX
    per_owner = document_corpus.shape[0]

    keys, values = passage_projection(
        document_corpus, document_rescale_factor, document_lookup_matrix, document_content_matrix
    )
    pieces, order = gather_tokens(symbol_activations, rank)

    groups = [[a * NX + b for b in range(NX)] for a in range(NZ)]
    plane_ids = lax.all_gather(
        document_choice_matrix.reshape(-1), "st", axis_index_groups=groups
    )

    def ranks_of(owner):
        place = jnp.arange(owner.shape[-1], dtype=jnp.int32)
        same = (owner[..., :, None] == owner[..., None, :]) & (place[:, None] > place[None, :])
        return jnp.sum(same.astype(jnp.int32), axis=-1)

    plane_owner = plane_ids // per_owner
    plane_rank = ranks_of(plane_owner)
    delta = jnp.arange(NZ, dtype=jnp.int32)
    holder = (z + delta) % NZ * NX + x
    hits = (plane_owner[None, :, None, :] == holder[:, None, None, None]) & (
        plane_rank[None, :, None, :] == jnp.arange(2, dtype=jnp.int32)[None, None, :, None]
    )
    index = jnp.sum(
        jnp.where(hits, (plane_ids % per_owner)[None, :, None, :], 0), axis=-1
    ).reshape(-1)

    ids = document_choice_matrix.reshape(-1)
    owner = ids // per_owner
    place = (
        (owner // NX - z + NZ) % NZ * (NX * 2) + owner % NX * 2 + ranks_of(owner)
    ).astype(jnp.int32)

    up_k, up_v, down_k, down_v = keys, values, keys, values
    stages = []
    held = [(0, keys, values)]
    for step in range(1, 4):
        up_k, down_k = along_z(up_k, 1), along_z(down_k, -1)
        up_v, down_v = along_z(up_v, 1), along_z(down_v, -1)
        held += [(NZ - step, up_k, up_v), (step, down_k, down_v)]
        stages.append(([d for d, _, _ in held], along_x(select(index, held))))
        held = []
    held = [(4, along_z(up_k, 1), along_z(down_v, -1))]
    stages.append(([4], along_x(select(index, held))))

    q, k, v, ask, mix, gates = token_projection(
        order,
        pieces,
        [
            memory_probe_matrix,
            memory_lookup_matrix,
            memory_content_matrix,
            document_probe_matrix,
            fetched_mixer_matrix,
        ],
        valve_matrix,
        valve_biases,
        added_decay_logit,
    )
    cell = cell_block(q, k, v, gates, facet_rescale_factor)
    scale = lax.dynamic_slice_in_dim(affinity_scaling, rank, 1, 0)
    return read_passages(place, scale, stages, ask, mix, cell)


def solution(mesh):
    return jax.shard_map(
        local,
        mesh=mesh,
        in_specs=(
            P("st", "tp"),
            P("st", None, None),
            P("st", None),
            P(None, "tp"),
            P(None, "tp"),
            P(None, "tp"),
            P(),
            P(),
            P("st", None),
            P("tp"),
            P(None, "tp"),
            P(None, "tp"),
            P(None, "tp"),
            P(),
            P(),
            P(None, "tp"),
        ),
        out_specs=P("st", "tp"),
        check_vma=False,
    )
```

```python
import functools

import jax
import jax.numpy as jnp
from jax import lax
from jax.experimental import pallas as pl
from jax.experimental.pallas import tpu as pltpu
from jax.sharding import PartitionSpec as P


FACETS = 8
LANES = 128
SEG = 128
EPS = 1e-06
EMPTY_LOG = -1e30
NZ = 8
NX = 4
PLACE_AT = NZ * NX * 2
HEAD_AT = PLACE_AT + 24
F32 = jnp.float32
BF16 = jnp.bfloat16


def dot(a, b, dims=((1,), (0,))):
    return lax.dot_general(a, b, (dims, ((), ())), preferred_element_type=F32)


def split_bf16(a):
    high = a.astype(BF16)
    return high, (a - high.astype(F32)).astype(BF16)


def passage_kernel(rows_ref, gain_ref, wk_ref, wv_ref, k_ref, v_ref, w_scr, n_scr):
    @pl.when(pl.program_id(0) == 0)
    def _():
        w_scr[:, :LANES] = wk_ref[...]
        w_scr[:, LANES:] = wv_ref[...]

    count, length, width = rows_ref.shape
    step = 16
    for p in range(count):
        for r in range(0, length, step):
            x = rows_ref[p, r : r + step, :].astype(F32)
            scale = lax.rsqrt(jnp.sum(x * x, axis=-1, keepdims=True) / width + EPS)
            n_scr[p * length + r : p * length + r + step, :] = (
                x * scale * gain_ref[...]
            ).astype(BF16)
    both = dot(n_scr[...], w_scr[...]).astype(BF16)
    k_ref[...] = both[:, :LANES].reshape(count, length, LANES)
    v_ref[...] = both[:, LANES:].reshape(count, length, LANES)


def passage_projection(corpus, gain, wk, wv):
    count, length, width = corpus.shape
    per = 4
    out = jax.ShapeDtypeStruct((count, length, LANES), BF16)
    return pl.pallas_call(
        passage_kernel,
        grid=(count // per,),
        in_specs=[
            pl.BlockSpec((per, length, width), lambda i: (i, 0, 0)),
            pl.BlockSpec((1, width), lambda i: (0, 0)),
            pl.BlockSpec((width, LANES), lambda i: (0, 0)),
            pl.BlockSpec((width, LANES), lambda i: (0, 0)),
        ],
        out_specs=[pl.BlockSpec((per, length, LANES), lambda i: (i, 0, 0))] * 2,
        out_shape=[out, out],
        scratch_shapes=[
            pltpu.VMEM((width, 2 * LANES), BF16),
            pltpu.VMEM((per * length, width), BF16),
        ],
        name="passage_projection",
    )(corpus, gain.reshape(1, width), wk, wv)


def token_kernel(plan_ref, bias_ref, *refs):
    pieces = refs[:8]
    weights = refs[8:13]
    valve_ref, decay_ref = refs[13:15]
    q_ref, k_ref, v_ref, ask_ref, mix_ref, gate_ref = refs[15:21]
    h_scr, w_scr, gate_scr, sems = refs[21:]
    head = plan_ref[HEAD_AT]
    y, core = head // 2, head % 2
    ranks = [(y + d) % 4 * 2 + core for d in (0, 3, 1, 2)]
    ranks += [(y + d) % 4 * 2 + 1 - core for d in (0, 3, 1, 2)]
    width = pieces[0].shape[1]
    copies = []
    for i, w in enumerate(weights):
        copies.append(
            pltpu.make_async_copy(w, w_scr.at[:, i * LANES : (i + 1) * LANES], sems.at[i])
        )
    for c in copies:
        c.start()
    for i, piece in enumerate(pieces):
        start = pl.multiple_of(ranks[i] * width, width)
        h_scr[:, pl.ds(start, width)] = piece[...]
    valve = valve_ref[...].astype(F32)
    rest = jnp.zeros((LANES - valve.shape[0], valve.shape[1]), F32)
    w_scr[:, 5 * LANES :] = jnp.concatenate([valve, rest], axis=0).T.astype(BF16)
    for c in copies:
        c.wait()
    h = h_scr[...]
    mg = dot(h, w_scr[:, 4 * LANES :])
    mix_ref[...] = mg[:, :LANES]
    gate_scr[...] = mg[:, LANES:].T
    qk = dot(h, w_scr[:, : 2 * LANES]).astype(BF16)
    q_ref[...] = qk[:, :LANES]
    k_ref[...] = qk[:, LANES:]
    va = dot(h, w_scr[:, 2 * LANES : 4 * LANES]).astype(BF16)
    v_ref[...] = va[:, :LANES]
    ask_ref[...] = va[:, LANES:]
    forget = gate_scr[pl.ds(FACETS + head, 1), :] + bias_ref[FACETS + head]
    gate_ref[0:1, :] = gate_scr[pl.ds(head, 1), :] + bias_ref[head]
    gate_ref[1:2, :] = (
        jnp.minimum(forget, 0.0)
        - jnp.log1p(jnp.exp(-jnp.abs(forget)))
        + decay_ref[pl.ds(head, 1), :]
    )


def token_projection(plan, pieces, weights, valve, bias, decay):
    rows = pieces[0].shape[0]
    width = valve.shape[0]
    half = jax.ShapeDtypeStruct((rows, LANES), BF16)
    vmem = pl.BlockSpec(memory_space=pltpu.VMEM)
    smem = pl.BlockSpec(memory_space=pltpu.SMEM)
    hbm = pl.BlockSpec(memory_space=pl.ANY)
    return pl.pallas_call(
        token_kernel,
        in_specs=[smem, smem] + [vmem] * 8 + [hbm] * 5 + [vmem] * 2,
        out_specs=[vmem] * 6,
        out_shape=[half] * 4
        + [jax.ShapeDtypeStruct((rows, LANES), F32), jax.ShapeDtypeStruct((2, rows), F32)],
        scratch_shapes=[
            pltpu.VMEM((rows, width), BF16),
            pltpu.VMEM((width, 6 * LANES), BF16),
            pltpu.VMEM((LANES, rows), F32),
            pltpu.SemaphoreType.DMA((5,)),
        ],
        name="token_projection",
    )(plan, bias, *pieces, *weights, valve.T, decay.T)


def cell_kernel(q_ref, k_ref, v_ref, gate_ref, facet_ref, out_ref):
    row = lax.broadcasted_iota(jnp.int32, (SEG, SEG), 0)
    col = lax.broadcasted_iota(jnp.int32, (SEG, SEG), 1)
    causal = row >= col
    eye = row == col
    scale = LANES ** (-0.5)

    def to_row(column):
        return jnp.sum(jnp.where(eye, column, 0.0), axis=0, keepdims=True)

    def to_col(line):
        return jnp.sum(jnp.where(eye, line, 0.0), axis=1, keepdims=True)

    memory = jnp.zeros((LANES, LANES), F32)
    normal = jnp.zeros((1, LANES), F32)
    stabilizer = jnp.full((1, 1), EMPTY_LOG, F32)
    for b in range(q_ref.shape[0] // SEG):
        part = slice(b * SEG, (b + 1) * SEG)
        q = q_ref[part, :]
        k = k_ref[part, :]
        v = v_ref[part, :]
        in_row = gate_ref[0:1, part]
        cum_col = jnp.sum(jnp.where(causal, gate_ref[1:2, part], 0.0), axis=1, keepdims=True)
        source = in_row - to_row(cum_col)
        log_weight = jnp.where(causal, cum_col + source, -jnp.inf)
        carried = cum_col + stabilizer
        peak = jnp.maximum(carried, jnp.max(log_weight, axis=1, keepdims=True))
        weight = jnp.exp(log_weight - peak)
        old = jnp.exp(carried - peak)
        logits = dot(q, k, ((1,), (1,))) * scale * weight
        high, low = split_bf16(logits)
        mem_high, mem_low = split_bf16(memory)
        numerator = old * (dot(q, mem_high) + dot(q, mem_low)) + (dot(high, v) + dot(low, v))
        denominator = old * jnp.sum(q.astype(F32) * normal, axis=1, keepdims=True) + jnp.sum(
            logits, axis=1, keepdims=True
        )
        cell = numerator / jnp.maximum(jnp.abs(denominator), jnp.exp(-peak))
        square = jnp.mean(cell * cell, axis=1, keepdims=True)
        out_ref[part, :] = cell * lax.rsqrt(square + EPS) * facet_ref[...]
        peak_last = peak[SEG - 1 :, :]
        cum_last = cum_col[SEG - 1 :, :]
        old_last = old[SEG - 1 :, :]
        last = jnp.exp(cum_last + to_col(source) - peak_last)
        weighted = k.astype(F32) * scale * last
        wk_high, wk_low = split_bf16(weighted)
        memory = old_last * memory + (
            dot(wk_high, v, ((0,), (0,))) + dot(wk_low, v, ((0,), (0,)))
        )
        normal = old_last * normal + jnp.sum(weighted, axis=0, keepdims=True)
        stabilizer = peak_last


def cell_block(q, k, v, gates, facet):
    vmem = pl.BlockSpec(memory_space=pltpu.VMEM)
    return pl.pallas_call(
        cell_kernel,
        in_specs=[vmem] * 5,
        out_specs=vmem,
        out_shape=jax.ShapeDtypeStruct(q.shape, F32),
        name="cell",
    )(q, k, v, gates, facet.reshape(1, LANES))


def select_kernel(deltas, plan_ref, *refs):
    arrays = refs[: 2 * len(deltas)]
    outs = refs[2 * len(deltas) :]
    for p, delta in enumerate(deltas):
        for turn in range(NX):
            for slot in range(2):
                at = plan_ref[(delta * NX + turn) * 2 + slot]
                for kind in range(2):
                    outs[turn][p, slot, kind] = arrays[2 * p + kind][at]


def select(plan, planes):
    deltas = [d for d, _, _ in planes]
    arrays = [a for _, k, v in planes for a in (k, v)]
    vmem = pl.BlockSpec(memory_space=pltpu.VMEM)
    _, length, lanes = arrays[0].shape
    out = jax.ShapeDtypeStruct((len(deltas), 2, 2, length, lanes), BF16)
    return pl.pallas_call(
        functools.partial(select_kernel, deltas),
        in_specs=[pl.BlockSpec(memory_space=pltpu.SMEM)] + [vmem] * len(arrays),
        out_specs=[vmem] * NX,
        out_shape=[out] * NX,
        name="select",
    )(plan, *arrays)


def read_kernel(groups, plan_ref, scale_ref, *refs):
    stages = refs[: len(groups) * NX]
    ask_ref, mix_ref, cell_ref, out_ref, kv_scr, k_scr, v_scr = refs[len(groups) * NX :]
    for n, deltas in enumerate(groups):
        for turn in range(NX):
            for p, delta in enumerate(deltas):
                kv_scr[delta, turn] = stages[n * NX + turn][p]
    row = lax.broadcasted_iota(jnp.int32, (SEG, SEG), 0)
    col = lax.broadcasted_iota(jnp.int32, (SEG, SEG), 1)
    eye = row == col
    length = k_scr.shape[0] // 4
    score_scale = scale_ref[plan_ref[HEAD_AT]] / LANES
    for b in range(out_ref.shape[0] // SEG):
        part = slice(b * SEG, (b + 1) * SEG)
        for i in range(4):
            place = plan_ref[PLACE_AT + b * 4 + i]
            delta = place // 8
            turn = (place // 2) % 4
            slot = place % 2
            rows = slice(i * length, (i + 1) * length)
            k_scr[rows, :] = kv_scr[delta, turn, slot, 0]
            v_scr[rows, :] = kv_scr[delta, turn, slot, 1]
        ask = ask_ref[part, :]
        keys = k_scr[...]
        ask32 = ask.astype(F32)
        key32 = keys.astype(F32)
        ask_scale = lax.rsqrt(jnp.mean(ask32 * ask32, axis=1, keepdims=True) + EPS)
        ask_row = jnp.sum(jnp.where(eye, ask_scale, 0.0), axis=0, keepdims=True)
        key_scale = lax.rsqrt(jnp.mean(key32 * key32, axis=1, keepdims=True) + EPS)
        scores = dot(keys, ask, ((1,), (1,))) * ask_row * key_scale * score_scale
        peak = jnp.max(scores, axis=0, keepdims=True)
        terms = jnp.exp(scores - peak)
        weights = (terms / jnp.sum(terms, axis=0, keepdims=True)).astype(BF16)
        retrieved = dot(weights, v_scr[...], ((0,), (0,)))
        gate = 1.0 / (1.0 + jnp.exp(-mix_ref[part, :]))
        out_ref[part, :] = (cell_ref[part, :] + gate * retrieved).astype(BF16)


def read_passages(plan, scale, stages, ask, mix, cell):
    groups = [d for d, _ in stages]
    arrays = [a for _, turned in stages for a in turned]
    length, lanes = arrays[0].shape[-2:]
    vmem = pl.BlockSpec(memory_space=pltpu.VMEM)
    smem = pl.BlockSpec(memory_space=pltpu.SMEM)
    hbm = pl.BlockSpec(memory_space=pl.ANY)
    return pl.pallas_call(
        functools.partial(read_kernel, groups),
        in_specs=[smem, smem] + [vmem] * (len(arrays) + 3),
        out_specs=vmem,
        out_shape=jax.ShapeDtypeStruct(ask.shape, BF16),
        scratch_shapes=[
            pltpu.VMEM((NZ, NX, 2, 2, length, lanes), BF16),
            pltpu.VMEM((4 * length, lanes), BF16),
            pltpu.VMEM((4 * length, lanes), BF16),
        ],
        name="read_passages",
    )(plan, scale, *arrays, ask, mix, cell)


def along_z(tensor, step):
    pairs = [(z * NX + x, (z + step) % NZ * NX + x) for z in range(NZ) for x in range(NX)]
    return lax.ppermute(tensor, "st", pairs)


def along_x(tensor, step):
    pairs = [(z * NX + x, z * NX + (x + step) % NX) for z in range(NZ) for x in range(NX)]
    return lax.ppermute(tensor, "st", pairs)


def to_tp(tensor, step, other):
    pairs = [
        (y * 2 + c, (y + step) % 4 * 2 + (1 - c if other else c)) for y in range(4) for c in range(2)
    ]
    return lax.ppermute(tensor, "tp", pairs)


def gather_tokens(tokens):
    own = [tokens] + [to_tp(tokens, d, False) for d in (1, -1, 2)]
    return own + [to_tp(p, 0, True) for p in own]


def body(
    symbol_activations,
    document_corpus,
    document_choice_matrix,
    memory_probe_matrix,
    memory_lookup_matrix,
    memory_content_matrix,
    valve_matrix,
    valve_biases,
    added_decay_logit,
    facet_rescale_factor,
    document_probe_matrix,
    document_lookup_matrix,
    document_content_matrix,
    document_rescale_factor,
    affinity_scaling,
    fetched_mixer_matrix,
):
    rank = lax.axis_index("tp")
    st = lax.axis_index("st")
    z, x = st // NX, st % NX
    per_owner = document_corpus.shape[0]
    ids = document_choice_matrix.reshape(-1)

    keys, values = passage_projection(
        document_corpus, document_rescale_factor, document_lookup_matrix, document_content_matrix
    )
    pieces = gather_tokens(symbol_activations)

    plane_ids = jnp.stack([ids] + [along_x(ids, -turn) for turn in range(1, NX)])

    def ranks_of(owner):
        place = jnp.arange(owner.shape[-1], dtype=jnp.int32)
        same = (owner[..., :, None] == owner[..., None, :]) & (place[:, None] > place[None, :])
        return jnp.sum(same.astype(jnp.int32), axis=-1)

    plane_owner = plane_ids // per_owner
    plane_rank = ranks_of(plane_owner)
    delta = jnp.arange(NZ, dtype=jnp.int32)
    holder = (z + delta) % NZ * NX + x
    hits = (plane_owner[None, :, None, :] == holder[:, None, None, None]) & (
        plane_rank[None, :, None, :] == jnp.arange(2, dtype=jnp.int32)[None, None, :, None]
    )
    index = jnp.sum(jnp.where(hits, (plane_ids % per_owner)[None, :, None, :], 0), axis=-1)
    owner = plane_owner[0]
    place = (owner // NX - z + NZ) % NZ * (NX * 2) + (x - owner + NZ * NX) % NX * 2 + plane_rank[0]
    plan = jnp.concatenate([index.reshape(-1), place, rank[None]]).astype(jnp.int32)

    up_k, up_v, down_k, down_v = keys, values, keys, values
    stages = []
    held = [(0, keys, values)]
    for step in range(1, 5):
        if step < 4:
            up_k, down_k = along_z(up_k, 1), along_z(down_k, -1)
            up_v, down_v = along_z(up_v, 1), along_z(down_v, -1)
            held += [(NZ - step, up_k, up_v), (step, down_k, down_v)]
        else:
            held = [(4, along_z(up_k, 1), along_z(down_v, -1))]
        picked = select(plan, held)
        turned = [picked[0]] + [along_x(picked[t], t) for t in range(1, NX)]
        stages.append(([d for d, _, _ in held], turned))
        held = []

    q, k, v, ask, mix, gates = token_projection(
        plan,
        pieces,
        [
            memory_probe_matrix,
            memory_lookup_matrix,
            memory_content_matrix,
            document_probe_matrix,
            fetched_mixer_matrix,
        ],
        valve_matrix,
        valve_biases,
        added_decay_logit,
    )
    cell = cell_block(q, k, v, gates, facet_rescale_factor)
    return read_passages(plan, affinity_scaling, stages, ask, mix, cell)


def solution(mesh):
    return jax.shard_map(
        body,
        mesh=mesh,
        in_specs=(
            P("st", "tp"),
            P("st", None, None),
            P("st", None),
            P(None, "tp"),
            P(None, "tp"),
            P(None, "tp"),
            P(),
            P(),
            P("st", None),
            P("tp"),
            P(None, "tp"),
            P(None, "tp"),
            P(None, "tp"),
            P(),
            P(),
            P(None, "tp"),
        ),
        out_specs=P("st", "tp"),
        check_vma=False,
    )
```

```python
import functools

import jax
import jax.numpy as jnp
from jax import lax
from jax.experimental import pallas as pl
from jax.experimental.pallas import tpu as pltpu
from jax.sharding import PartitionSpec as P


FACETS = 8
LANES = 128
SEG = 128
EPS = 1e-06
EMPTY_LOG = -1e30
NZ = 8
NX = 4
PLACE_AT = 32
F32 = jnp.float32
BF16 = jnp.bfloat16


def dot(a, b, dims=((1,), (0,))):
    return lax.dot_general(a, b, (dims, ((), ())), preferred_element_type=F32)


def split_bf16(a):
    high = a.astype(BF16)
    return high, (a - high.astype(F32)).astype(BF16)


def normalize(rows_ref, gain_ref, n_scr, first, count):
    _, length, width = rows_ref.shape
    step = 16
    for p in range(first, first + count):
        for r in range(0, length, step):
            x = rows_ref[p, r : r + step, :].astype(F32)
            scale = lax.rsqrt(jnp.sum(x * x, axis=-1, keepdims=True) / width + EPS)
            n_scr[p * length + r : p * length + r + step, :] = (
                x * scale * gain_ref[...]
            ).astype(BF16)


def project(n_scr, w, kv_ref, first, count):
    length = kv_ref.shape[2]
    both = dot(n_scr[first * length : (first + count) * length, :], w).astype(BF16)
    kv_ref[first : first + count, 0] = both[:, :LANES].reshape(count, length, LANES)
    kv_ref[first : first + count, 1] = both[:, LANES:].reshape(count, length, LANES)


def first_kernel(corpus_ref, line_ref, wk_ref, wv_ref, *refs):
    kv_ref, rest_ref, w_ref, gain_ref, rows, n_scr, sems = refs
    half = rows.shape[0]
    group = half // 2

    def copy(n, source, target):
        return pltpu.make_async_copy(source, target, sems.at[n])

    own = [copy(p, corpus_ref.at[p], rows.at[p]) for p in range(half)]
    later = [copy(half + p, corpus_ref.at[half + p], rest_ref.at[p]) for p in range(half)]
    weights = [
        copy(2 * half, wk_ref, w_ref.at[:, :LANES]),
        copy(2 * half + 1, wv_ref, w_ref.at[:, LANES:]),
    ]
    gain = copy(2 * half + 2, line_ref, gain_ref)
    for c in [gain] + own[:group] + weights + own[group:]:
        c.start()
    for c in [gain] + own[:group]:
        c.wait()
    normalize(rows, gain_ref, n_scr, 0, group)
    for c in weights + own[group:]:
        c.wait()
    for c in later:
        c.start()
    project(n_scr, w_ref[...], kv_ref, 0, group)
    normalize(rows, gain_ref, n_scr, group, group)
    project(n_scr, w_ref[...], kv_ref, group, group)
    for c in later:
        c.wait()


def second_kernel(rows_ref, gain_ref, w_ref, *refs):
    weights, valve_ref = refs[:5], refs[5]
    kv_ref, joined_ref, n_scr, sems = refs[6:]
    copies = [
        pltpu.make_async_copy(w, joined_ref.at[:, i * LANES : (i + 1) * LANES], sems.at[i])
        for i, w in enumerate(weights)
    ]
    for c in copies:
        c.start()
    valve = valve_ref[...].astype(F32)
    rest = jnp.zeros((valve.shape[1], LANES - valve.shape[0]), BF16)
    joined_ref[:, 5 * LANES :] = jnp.concatenate([valve.T.astype(BF16), rest], axis=1)
    half = rows_ref.shape[0]
    group = half // 2
    normalize(rows_ref, gain_ref, n_scr, 0, group)
    project(n_scr, w_ref[...], kv_ref, 0, group)
    normalize(rows_ref, gain_ref, n_scr, group, group)
    project(n_scr, w_ref[...], kv_ref, group, group)
    for c in copies:
        c.wait()


def in_hbm(array):
    return pltpu.with_memory_space_constraint(array, pltpu.HBM)


def in_vmem(array):
    return pltpu.with_memory_space_constraint(array, pltpu.VMEM)


def passage_projection(corpus, gain, wk, wv, weights, valve):
    count, length, width = corpus.shape
    half = count // 2
    vmem = pl.BlockSpec(memory_space=pltpu.VMEM)
    hbm = pl.BlockSpec(memory_space=pltpu.HBM)
    kv = jax.ShapeDtypeStruct((half, 2, length, LANES), BF16)
    normed = pltpu.VMEM((half * length, width), BF16)
    gain = gain.reshape(1, width)
    first, rows, w, gain = pl.pallas_call(
        first_kernel,
        in_specs=[hbm] * 4,
        out_specs=[vmem] * 4,
        out_shape=[
            kv,
            jax.ShapeDtypeStruct((half, length, width), BF16),
            jax.ShapeDtypeStruct((width, 2 * LANES), BF16),
            jax.ShapeDtypeStruct((1, width), F32),
        ],
        scratch_shapes=[
            pltpu.VMEM((half, length, width), BF16),
            normed,
            pltpu.SemaphoreType.DMA((2 * half + 3,)),
        ],
        compiler_params=pltpu.CompilerParams(vmem_limit_bytes=20 << 20),
        name="first_half",
    )(in_hbm(corpus), in_hbm(gain), in_hbm(wk), in_hbm(wv))
    second, joined = pl.pallas_call(
        second_kernel,
        in_specs=[vmem] * 3 + [hbm] * 5 + [vmem],
        out_specs=[vmem] * 2,
        out_shape=[kv, jax.ShapeDtypeStruct((width, 6 * LANES), BF16)],
        scratch_shapes=[normed, pltpu.SemaphoreType.DMA((5,))],
        compiler_params=pltpu.CompilerParams(vmem_limit_bytes=20 << 20),
        name="second_half",
    )(rows, gain, w, *map(in_hbm, weights), valve.T)
    return [in_vmem(first), in_vmem(second)], joined


def bits(size):
    assert size & (size - 1) == 0
    return size.bit_length() - 1


def shift(value, size):
    return lax.shift_right_logical(value, jnp.int32(bits(size)))


def low(value, size):
    return value & (size - 1)


def ranks(owner, reads):
    rank = jnp.zeros(owner.shape, jnp.int32)
    for back in range(1, reads):
        rank = rank + jnp.where(pltpu.roll(owner, back, 1) == owner, 1, 0)
    return rank


def owners(ids, per_owner, reads):
    lane = lax.broadcasted_iota(jnp.int32, ids.shape, 1)
    return lane, jnp.where(lane < reads, shift(ids, per_owner), -1)


def add_columns(plan, first, target, lane, owner, rank, within):
    for slot in range(2):
        found = jnp.where((owner == target) & (rank == slot), within, 0)
        column = jnp.sum(found, axis=1, keepdims=True)
        plan = jnp.where(lane == first + slot, column, plan)
    return plan


def plan_kernel(per_owner, *refs):
    readers = refs[:NX]
    out_ref, ids_ref = refs[NX:]
    st = lax.axis_index("st")
    z, x = shift(st, NX), low(st, NX)
    per_block, blocks = readers[0].shape
    reads = per_block * blocks
    ids_ref[...] = jnp.zeros(ids_ref.shape, jnp.int32)
    for turn, reader in enumerate(readers):
        for n in range(per_block):
            ids_ref[turn : turn + 1, n * blocks : (n + 1) * blocks] = reader[n : n + 1, :]
    ids = ids_ref[...]
    lane, owner = owners(ids, per_owner, reads)
    rank = ranks(owner, reads)
    delta = low(shift(owner, NX) - z, NZ)
    turn = low(x - owner, NX)
    plan = pltpu.roll((delta * NX + turn) * 2 + rank, PLACE_AT, 1)
    for source in range(NZ):
        target = low(z + source, NZ) * NX + x
        plan = add_columns(plan, source * 2, target, lane, owner, rank, low(ids, per_owner))
    out_ref[...] = plan


def far_plan_kernel(per_owner, reads, above_ref, below_ref, out_ref):
    st = lax.axis_index("st")
    z, x = shift(st, NX), low(st, NX)
    plan = jnp.zeros(out_ref.shape, jnp.int32)
    for n, (ids_ref, source) in enumerate(((above_ref, -3), (below_ref, 3))):
        ids = ids_ref[...]
        lane, owner = owners(ids, per_owner, reads)
        target = low(z + source, NZ) * NX + x
        rank = ranks(owner, reads)
        plan = add_columns(plan, n * 2, target, lane, owner, rank, low(ids, per_owner))
    out_ref[...] = plan


def plan_call(kernel, arrays, outs):
    vmem = pl.BlockSpec(memory_space=pltpu.VMEM)
    return pl.pallas_call(
        kernel,
        in_specs=[vmem] * len(arrays),
        out_specs=[vmem] * outs,
        out_shape=[jax.ShapeDtypeStruct((NX * 2, LANES), jnp.int32)] * outs,
        compiler_params=pltpu.CompilerParams(vmem_limit_bytes=2 << 20),
    )(*arrays)


def token_kernel(bias_ref, *refs):
    pieces = refs[:8]
    w_ref, decay_ref = refs[8:10]
    q_ref, k_ref, v_ref, ask_ref, mix_ref, gate_ref = refs[10:16]
    h_scr, gate_scr, decay_scr, sem = refs[16:]
    decay = pltpu.make_async_copy(decay_ref, decay_scr, sem)
    decay.start()
    head = lax.axis_index("tp")
    y, core = shift(head, 2), low(head, 2)
    ranks = [low(y + d, 4) * 2 + core for d in (0, 3, 1, 2)]
    ranks += [low(y + d, 4) * 2 + 1 - core for d in (0, 3, 1, 2)]
    width = pieces[0].shape[1]
    for i, piece in enumerate(pieces):
        start = pl.multiple_of(ranks[i] * width, width)
        h_scr[:, pl.ds(start, width)] = piece[...]
    h = h_scr[...]
    mg = dot(h, w_ref[:, 4 * LANES :])
    mix_ref[...] = mg[:, :LANES]
    gate_scr[...] = mg[:, LANES:].T
    qk = dot(h, w_ref[:, : 2 * LANES]).astype(BF16)
    q_ref[...] = qk[:, :LANES]
    k_ref[...] = qk[:, LANES:]
    va = dot(h, w_ref[:, 2 * LANES : 4 * LANES]).astype(BF16)
    v_ref[...] = va[:, :LANES]
    ask_ref[...] = va[:, LANES:]
    decay.wait()
    forget = gate_scr[pl.ds(FACETS + head, 1), :] + bias_ref[FACETS + head]
    gate_ref[0:1, :] = gate_scr[pl.ds(head, 1), :] + bias_ref[head]
    gate_ref[1:2, :] = (
        jnp.minimum(forget, 0.0)
        - jnp.log1p(jnp.exp(-jnp.abs(forget)))
        + decay_scr[pl.ds(head, 1), :]
    )


def token_projection(pieces, weights, bias, decay):
    rows = pieces[0].shape[0]
    half = jax.ShapeDtypeStruct((rows, LANES), BF16)
    vmem = pl.BlockSpec(memory_space=pltpu.VMEM)
    return pl.pallas_call(
        token_kernel,
        in_specs=[pl.BlockSpec(memory_space=pltpu.SMEM)]
        + [vmem] * 9
        + [pl.BlockSpec(memory_space=pltpu.HBM)],
        out_specs=[vmem] * 6,
        out_shape=[half] * 4
        + [jax.ShapeDtypeStruct((rows, LANES), F32), jax.ShapeDtypeStruct((2, rows), F32)],
        scratch_shapes=[
            pltpu.VMEM((rows, weights.shape[0]), BF16),
            pltpu.VMEM((LANES, rows), F32),
            pltpu.VMEM((FACETS, rows), F32),
            pltpu.SemaphoreType.DMA,
        ],
        compiler_params=pltpu.CompilerParams(vmem_limit_bytes=20 << 20),
        name="token_projection",
    )(bias, *pieces, weights, in_hbm(decay.T))


def cell_kernel(q_ref, k_ref, v_ref, gate_ref, facet_ref, out_ref):
    row = lax.broadcasted_iota(jnp.int32, (SEG, SEG), 0)
    col = lax.broadcasted_iota(jnp.int32, (SEG, SEG), 1)
    causal = row >= col
    eye = row == col
    scale = LANES ** (-0.5)

    def to_row(column):
        return jnp.sum(jnp.where(eye, column, 0.0), axis=0, keepdims=True)

    def to_col(line):
        return jnp.sum(jnp.where(eye, line, 0.0), axis=1, keepdims=True)

    memory = jnp.zeros((LANES, LANES), F32)
    normal = jnp.zeros((1, LANES), F32)
    stabilizer = jnp.full((1, 1), EMPTY_LOG, F32)
    for b in range(q_ref.shape[0] // SEG):
        part = slice(b * SEG, (b + 1) * SEG)
        q = q_ref[part, :]
        k = k_ref[part, :]
        v = v_ref[part, :]
        in_row = gate_ref[0:1, part]
        cum_col = jnp.sum(jnp.where(causal, gate_ref[1:2, part], 0.0), axis=1, keepdims=True)
        source = in_row - to_row(cum_col)
        log_weight = jnp.where(causal, cum_col + source, -jnp.inf)
        carried = cum_col + stabilizer
        peak = jnp.maximum(carried, jnp.max(log_weight, axis=1, keepdims=True))
        weight = jnp.exp(log_weight - peak)
        old = jnp.exp(carried - peak)
        logits = dot(q, k, ((1,), (1,))) * scale * weight
        high, low = split_bf16(logits)
        mem_high, mem_low = split_bf16(memory)
        numerator = old * (dot(q, mem_high) + dot(q, mem_low)) + (dot(high, v) + dot(low, v))
        denominator = old * jnp.sum(q.astype(F32) * normal, axis=1, keepdims=True) + jnp.sum(
            logits, axis=1, keepdims=True
        )
        cell = numerator / jnp.maximum(jnp.abs(denominator), jnp.exp(-peak))
        square = jnp.mean(cell * cell, axis=1, keepdims=True)
        out_ref[part, :] = cell * lax.rsqrt(square + EPS) * facet_ref[...]
        peak_last = peak[SEG - 1 :, :]
        cum_last = cum_col[SEG - 1 :, :]
        old_last = old[SEG - 1 :, :]
        last = jnp.exp(cum_last + to_col(source) - peak_last)
        weighted = k.astype(F32) * scale * last
        wk_high, wk_low = split_bf16(weighted)
        memory = old_last * memory + (
            dot(wk_high, v, ((0,), (0,))) + dot(wk_low, v, ((0,), (0,)))
        )
        normal = old_last * normal + jnp.sum(weighted, axis=0, keepdims=True)
        stabilizer = peak_last


def cell_block(q, k, v, gates, facet):
    vmem = pl.BlockSpec(memory_space=pltpu.VMEM)
    return pl.pallas_call(
        cell_kernel,
        in_specs=[vmem] * 5,
        out_specs=vmem,
        out_shape=jax.ShapeDtypeStruct(q.shape, F32),
        compiler_params=pltpu.CompilerParams(vmem_limit_bytes=8 << 20),
        name="cell",
    )(q, k, v, gates, facet.reshape(1, LANES))


def passage(halves, at):
    first, second = (ref[low(at, ref.shape[0])] for ref in halves)
    return jnp.where(at < halves[0].shape[0], first, second)


def select_kernel(deltas, plan_ref, *refs):
    arrays, outs = refs[: 2 * len(deltas)], refs[2 * len(deltas) :]
    for p, delta in enumerate(deltas):
        for turn in range(NX):
            for slot in range(2):
                at = plan_ref[turn, delta * 2 + slot]
                outs[turn][p, slot] = passage(arrays[2 * p : 2 * p + 2], at)


def far_kernel(plan_ref, *refs):
    arrays, outs = refs[:4], refs[4:]
    for turn in range(NX):
        way = turn // 2
        for slot in range(2):
            at = plan_ref[turn, way * 2 + slot]
            outs[turn][slot] = passage(arrays[way * 2 : way * 2 + 2], at)


def pick(kernel, plan, arrays, planes):
    vmem = pl.BlockSpec(memory_space=pltpu.VMEM)
    out = jax.ShapeDtypeStruct(planes + (2,) + arrays[0].shape[1:], BF16)
    return pl.pallas_call(
        kernel,
        in_specs=[pl.BlockSpec(memory_space=pltpu.SMEM)] + [vmem] * len(arrays),
        out_specs=[vmem] * NX,
        out_shape=[out] * NX,
        compiler_params=pltpu.CompilerParams(vmem_limit_bytes=8 << 20),
    )(plan, *arrays)


def select(plan, held):
    deltas = [delta for delta, _, _ in held]
    arrays = [a for _, first, second in held for a in (first, second)]
    kernel = functools.partial(select_kernel, deltas)
    return deltas, pick(kernel, plan, arrays, (len(deltas),))


def read_kernel(groups, plan_ref, scale_ref, *refs):
    across = refs[: len(groups) * NX]
    far = refs[len(groups) * NX : (len(groups) + 1) * NX]
    ask_ref, mix_ref, cell_ref, out_ref, kv_scr, k_scr, v_scr = refs[(len(groups) + 1) * NX :]
    for n, deltas in enumerate(groups):
        for turn in range(NX):
            for p, delta in enumerate(deltas):
                kv_scr[delta, turn] = across[n * NX + turn][p]
    for turn in range(NX):
        kv_scr[NZ // 2, turn] = far[turn][...]
    row = lax.broadcasted_iota(jnp.int32, (SEG, SEG), 0)
    col = lax.broadcasted_iota(jnp.int32, (SEG, SEG), 1)
    eye = row == col
    length = k_scr.shape[0] // 4
    score_scale = scale_ref[lax.axis_index("tp")] / LANES
    blocks = out_ref.shape[0] // SEG
    for b in range(blocks):
        part = slice(b * SEG, (b + 1) * SEG)
        for i in range(4):
            place = plan_ref[0, PLACE_AT + i * blocks + b]
            delta = shift(place, NX * 2)
            turn = low(shift(place, 2), NX)
            slot = low(place, 2)
            rows = slice(i * length, (i + 1) * length)
            k_scr[rows, :] = kv_scr[delta, turn, slot, 0]
            v_scr[rows, :] = kv_scr[delta, turn, slot, 1]
        ask = ask_ref[part, :]
        keys = k_scr[...]
        ask32 = ask.astype(F32)
        key32 = keys.astype(F32)
        ask_scale = lax.rsqrt(jnp.mean(ask32 * ask32, axis=1, keepdims=True) + EPS)
        ask_row = jnp.sum(jnp.where(eye, ask_scale, 0.0), axis=0, keepdims=True)
        key_scale = lax.rsqrt(jnp.mean(key32 * key32, axis=1, keepdims=True) + EPS)
        scores = dot(keys, ask, ((1,), (1,))) * ask_row * key_scale * score_scale
        peak = jnp.max(scores, axis=0, keepdims=True)
        terms = jnp.exp(scores - peak)
        weights = (terms / jnp.sum(terms, axis=0, keepdims=True)).astype(BF16)
        retrieved = dot(weights, v_scr[...], ((0,), (0,)))
        gate = 1.0 / (1.0 + jnp.exp(-mix_ref[part, :]))
        out_ref[part, :] = (cell_ref[part, :] + gate * retrieved).astype(BF16)


def read_passages(plan, scale, stages, far, ask, mix, cell):
    groups = [d for d, _ in stages]
    arrays = [a for _, turned in stages for a in turned] + far
    length, lanes = arrays[0].shape[-2:]
    vmem = pl.BlockSpec(memory_space=pltpu.VMEM)
    smem = pl.BlockSpec(memory_space=pltpu.SMEM)
    hbm = pl.BlockSpec(memory_space=pltpu.HBM)
    return pl.pallas_call(
        functools.partial(read_kernel, groups),
        in_specs=[smem, smem] + [vmem] * (len(arrays) + 3),
        out_specs=vmem,
        out_shape=jax.ShapeDtypeStruct(ask.shape, BF16),
        scratch_shapes=[
            pltpu.VMEM((NZ, NX, 2, 2, length, lanes), BF16),
            pltpu.VMEM((4 * length, lanes), BF16),
            pltpu.VMEM((4 * length, lanes), BF16),
        ],
        compiler_params=pltpu.CompilerParams(vmem_limit_bytes=16 << 20),
        name="read_passages",
    )(plan, scale, *arrays, ask, mix, cell)


def send(tensor, up, turn):
    pairs = [
        (z * NX + x, (z + up) % NZ * NX + (x + turn) % NX) for z in range(NZ) for x in range(NX)
    ]
    return lax.ppermute(tensor, "st", pairs)


def along_x(picked):
    return [picked[0]] + [send(picked[t], 0, t) for t in range(1, NX)]


def to_tp(tensor, step, other):
    pairs = [
        (y * 2 + c, (y + step) % 4 * 2 + (1 - c if other else c)) for y in range(4) for c in range(2)
    ]
    return lax.ppermute(tensor, "tp", pairs)


def gather_tokens(tokens):
    own = [tokens] + [to_tp(tokens, d, False) for d in (1, -1, 2)]
    return own + [to_tp(p, 0, True) for p in own]


def body(
    symbol_activations,
    document_corpus,
    document_choice_matrix,
    memory_probe_matrix,
    memory_lookup_matrix,
    memory_content_matrix,
    valve_matrix,
    valve_biases,
    added_decay_logit,
    facet_rescale_factor,
    document_probe_matrix,
    document_lookup_matrix,
    document_content_matrix,
    document_rescale_factor,
    affinity_scaling,
    fetched_mixer_matrix,
):
    per_owner = document_corpus.shape[0]
    ids = document_choice_matrix.T

    own, joined = passage_projection(
        document_corpus,
        document_rescale_factor,
        document_lookup_matrix,
        document_content_matrix,
        [
            memory_probe_matrix,
            memory_lookup_matrix,
            memory_content_matrix,
            document_probe_matrix,
            fetched_mixer_matrix,
        ],
        valve_matrix,
    )
    pieces = gather_tokens(symbol_activations)
    readers = [ids] + [send(ids, 0, -turn) for turn in range(1, NX)]
    kernel = functools.partial(plan_kernel, per_owner)
    plan, plane_ids = plan_call(kernel, readers, 2)
    near = (send(plane_ids, -1, 0), send(plane_ids, 1, 0))
    kernel = functools.partial(far_plan_kernel, per_owner, ids.size)
    (far_plan,) = plan_call(kernel, near, 1)

    up, down = list(own), list(own)
    held = [(0, *own)]
    stages = []
    for step in range(1, 4):
        for n in range(2):
            up[n] = in_vmem(send(up[n], 1, 0))
            down[n] = in_vmem(send(down[n], -1, 0))
        held += [(NZ - step, *up), (step, *down)]
        deltas, picked = select(plan, held)
        held = []
        stages.append((deltas, along_x(picked)))
    far = pick(far_kernel, far_plan, [*up, *down], ())
    far = [send(far[t], 1 if t < 2 else -1, t) for t in range(NX)]

    q, k, v, ask, mix, gates = token_projection(pieces, joined, valve_biases, added_decay_logit)
    cell = cell_block(q, k, v, gates, facet_rescale_factor)
    return read_passages(plan, affinity_scaling, stages, far, ask, mix, cell)


def solution(mesh):
    return jax.shard_map(
        body,
        mesh=mesh,
        in_specs=(
            P("st", "tp"),
            P("st", None, None),
            P("st", None),
            P(None, "tp"),
            P(None, "tp"),
            P(None, "tp"),
            P(),
            P(),
            P("st", None),
            P("tp"),
            P(None, "tp"),
            P(None, "tp"),
            P(None, "tp"),
            P(),
            P(),
            P(None, "tp"),
        ),
        out_specs=P("st", "tp"),
        check_vma=False,
    )
```

```python
import functools

import jax
import jax.numpy as jnp
from jax import lax
from jax.experimental import pallas as pl
from jax.experimental.pallas import tpu as pltpu
from jax.sharding import PartitionSpec as P


FACETS = 8
LANES = 128
SEG = 128
EPS = 1e-06
EMPTY_LOG = -1e30
NZ = 8
NX = 4
PLACE_AT = 32
F32 = jnp.float32
BF16 = jnp.bfloat16


def dot(a, b, dims=((1,), (0,))):
    return lax.dot_general(a, b, (dims, ((), ())), preferred_element_type=F32)


def split_bf16(a):
    high = a.astype(BF16)
    return high, (a - high.astype(F32)).astype(BF16)


def normalize(rows_ref, gain_ref, n_scr, first, count):
    _, length, width = rows_ref.shape
    step = 16
    for p in range(first, first + count):
        for r in range(0, length, step):
            x = rows_ref[p, r : r + step, :].astype(F32)
            scale = lax.rsqrt(jnp.sum(x * x, axis=-1, keepdims=True) / width + EPS)
            n_scr[p * length + r : p * length + r + step, :] = (
                x * scale * gain_ref[...]
            ).astype(BF16)


def project(n_scr, w, kv_ref, first, count):
    length = kv_ref.shape[2]
    both = dot(n_scr[first * length : (first + count) * length, :], w).astype(BF16)
    kv_ref[first : first + count, 0] = both[:, :LANES].reshape(count, length, LANES)
    kv_ref[first : first + count, 1] = both[:, LANES:].reshape(count, length, LANES)


def first_kernel(corpus_ref, line_ref, wk_ref, wv_ref, *refs):
    kv_ref, rest_ref, w_ref, gain_ref, rows, n_scr, sems = refs
    half = rows.shape[0]
    group = half // 2

    def copy(n, source, target):
        return pltpu.make_async_copy(source, target, sems.at[n])

    own = [copy(p, corpus_ref.at[p], rows.at[p]) for p in range(half)]
    later = [copy(half + p, corpus_ref.at[half + p], rest_ref.at[p]) for p in range(half)]
    weights = [
        copy(2 * half, wk_ref, w_ref.at[:, :LANES]),
        copy(2 * half + 1, wv_ref, w_ref.at[:, LANES:]),
    ]
    gain = copy(2 * half + 2, line_ref, gain_ref)
    for c in [gain] + own[:group] + weights + own[group:]:
        c.start()
    for c in [gain] + own[:group]:
        c.wait()
    normalize(rows, gain_ref, n_scr, 0, group)
    for c in weights + own[group:]:
        c.wait()
    for c in later:
        c.start()
    project(n_scr, w_ref[...], kv_ref, 0, group)
    normalize(rows, gain_ref, n_scr, group, group)
    project(n_scr, w_ref[...], kv_ref, group, group)
    for c in later:
        c.wait()


def second_kernel(rows_ref, gain_ref, w_ref, *refs):
    weights, valve_ref = refs[:5], refs[5]
    kv_ref, joined_ref, n_scr, sems = refs[6:]
    copies = [
        pltpu.make_async_copy(w, joined_ref.at[:, i * LANES : (i + 1) * LANES], sems.at[i])
        for i, w in enumerate(weights)
    ]
    for c in copies:
        c.start()
    valve = valve_ref[...].astype(F32)
    rest = jnp.zeros((valve.shape[1], LANES - valve.shape[0]), BF16)
    joined_ref[:, 5 * LANES :] = jnp.concatenate([valve.T.astype(BF16), rest], axis=1)
    half = rows_ref.shape[0]
    group = half // 2
    normalize(rows_ref, gain_ref, n_scr, 0, group)
    project(n_scr, w_ref[...], kv_ref, 0, group)
    normalize(rows_ref, gain_ref, n_scr, group, group)
    project(n_scr, w_ref[...], kv_ref, group, group)
    for c in copies:
        c.wait()


def in_hbm(array):
    return pltpu.with_memory_space_constraint(array, pltpu.HBM)


def in_vmem(array):
    return pltpu.with_memory_space_constraint(array, pltpu.VMEM)


def passage_projection(corpus, gain, wk, wv, weights, valve):
    count, length, width = corpus.shape
    half = count // 2
    vmem = pl.BlockSpec(memory_space=pltpu.VMEM)
    hbm = pl.BlockSpec(memory_space=pltpu.HBM)
    kv = jax.ShapeDtypeStruct((half, 2, length, LANES), BF16)
    normed = pltpu.VMEM((half * length, width), BF16)
    gain = gain.reshape(1, width)
    first, rows, w, gain = pl.pallas_call(
        first_kernel,
        in_specs=[hbm] * 4,
        out_specs=[vmem] * 4,
        out_shape=[
            kv,
            jax.ShapeDtypeStruct((half, length, width), BF16),
            jax.ShapeDtypeStruct((width, 2 * LANES), BF16),
            jax.ShapeDtypeStruct((1, width), F32),
        ],
        scratch_shapes=[
            pltpu.VMEM((half, length, width), BF16),
            normed,
            pltpu.SemaphoreType.DMA((2 * half + 3,)),
        ],
        compiler_params=pltpu.CompilerParams(vmem_limit_bytes=20 << 20),
        name="first_half",
    )(in_hbm(corpus), in_hbm(gain), in_hbm(wk), in_hbm(wv))
    second, joined = pl.pallas_call(
        second_kernel,
        in_specs=[vmem] * 3 + [hbm] * 5 + [vmem],
        out_specs=[vmem] * 2,
        out_shape=[kv, jax.ShapeDtypeStruct((width, 6 * LANES), BF16)],
        scratch_shapes=[normed, pltpu.SemaphoreType.DMA((5,))],
        compiler_params=pltpu.CompilerParams(vmem_limit_bytes=20 << 20),
        name="second_half",
    )(rows, gain, w, *map(in_hbm, weights), valve.T)
    return [in_vmem(first), in_vmem(second)], joined


def bits(size):
    assert size & (size - 1) == 0
    return size.bit_length() - 1


def shift(value, size):
    return lax.shift_right_logical(value, jnp.int32(bits(size)))


def low(value, size):
    return value & (size - 1)


def ranks(owner, reads):
    rank = jnp.zeros(owner.shape, jnp.int32)
    for back in range(1, reads):
        rank = rank + jnp.where(pltpu.roll(owner, back, 1) == owner, 1, 0)
    return rank


def owners(ids, per_owner, reads):
    lane = lax.broadcasted_iota(jnp.int32, ids.shape, 1)
    return lane, jnp.where(lane < reads, shift(ids, per_owner), -1)


def add_columns(plan, first, target, lane, owner, rank, within):
    for slot in range(2):
        found = jnp.where((owner == target) & (rank == slot), within, 0)
        column = jnp.sum(found, axis=1, keepdims=True)
        plan = jnp.where(lane == first + slot, column, plan)
    return plan


def plan_kernel(per_owner, *refs):
    readers = refs[:NX]
    out_ref, ids_ref = refs[NX:]
    st = lax.axis_index("st")
    z, x = shift(st, NX), low(st, NX)
    per_block, blocks = readers[0].shape
    reads = per_block * blocks
    ids_ref[...] = jnp.zeros(ids_ref.shape, jnp.int32)
    for turn, reader in enumerate(readers):
        for n in range(per_block):
            ids_ref[turn : turn + 1, n * blocks : (n + 1) * blocks] = reader[n : n + 1, :]
    ids = ids_ref[...]
    lane, owner = owners(ids, per_owner, reads)
    rank = ranks(owner, reads)
    delta = low(shift(owner, NX) - z, NZ)
    turn = low(x - owner, NX)
    plan = pltpu.roll((delta * NX + turn) * 2 + rank, PLACE_AT, 1)
    for source in range(NZ):
        target = low(z + source, NZ) * NX + x
        plan = add_columns(plan, source * 2, target, lane, owner, rank, low(ids, per_owner))
    out_ref[...] = plan


def far_plan_kernel(per_owner, reads, above_ref, below_ref, out_ref):
    st = lax.axis_index("st")
    z, x = shift(st, NX), low(st, NX)
    plan = jnp.zeros(out_ref.shape, jnp.int32)
    for n, (ids_ref, source) in enumerate(((above_ref, -3), (below_ref, 3))):
        ids = ids_ref[...]
        lane, owner = owners(ids, per_owner, reads)
        target = low(z + source, NZ) * NX + x
        rank = ranks(owner, reads)
        plan = add_columns(plan, n * 2, target, lane, owner, rank, low(ids, per_owner))
    out_ref[...] = plan


def plan_call(kernel, arrays, outs):
    vmem = pl.BlockSpec(memory_space=pltpu.VMEM)
    return pl.pallas_call(
        kernel,
        in_specs=[vmem] * len(arrays),
        out_specs=[vmem] * outs,
        out_shape=[jax.ShapeDtypeStruct((NX * 2, LANES), jnp.int32)] * outs,
        compiler_params=pltpu.CompilerParams(vmem_limit_bytes=2 << 20),
    )(*arrays)


def token_kernel(bias_ref, *refs):
    pieces = refs[:8]
    w_ref, decay_ref = refs[8:10]
    q_ref, k_ref, v_ref, ask_ref, mix_ref, gate_ref = refs[10:16]
    h_scr, gate_scr, decay_scr, sem = refs[16:]
    decay = pltpu.make_async_copy(decay_ref, decay_scr, sem)
    decay.start()
    head = lax.axis_index("tp")
    y, core = shift(head, 2), low(head, 2)
    ranks = [low(y + d, 4) * 2 + core for d in (0, 3, 1, 2)]
    ranks += [low(y + d, 4) * 2 + 1 - core for d in (0, 3, 1, 2)]
    width = pieces[0].shape[1]
    for i, piece in enumerate(pieces):
        start = pl.multiple_of(ranks[i] * width, width)
        h_scr[:, pl.ds(start, width)] = piece[...]
    h = h_scr[...]
    mg = dot(h, w_ref[:, 4 * LANES :])
    mix_ref[...] = mg[:, :LANES]
    gate_scr[...] = mg[:, LANES:].T
    qk = dot(h, w_ref[:, : 2 * LANES]).astype(BF16)
    q_ref[...] = qk[:, :LANES]
    k_ref[...] = qk[:, LANES:]
    va = dot(h, w_ref[:, 2 * LANES : 4 * LANES]).astype(BF16)
    v_ref[...] = va[:, :LANES]
    ask_ref[...] = va[:, LANES:]
    decay.wait()
    forget = gate_scr[pl.ds(FACETS + head, 1), :] + bias_ref[FACETS + head]
    gate_ref[0:1, :] = gate_scr[pl.ds(head, 1), :] + bias_ref[head]
    gate_ref[1:2, :] = (
        jnp.minimum(forget, 0.0)
        - jnp.log1p(jnp.exp(-jnp.abs(forget)))
        + decay_scr[pl.ds(head, 1), :]
    )


def token_projection(pieces, weights, bias, decay):
    rows = pieces[0].shape[0]
    half = jax.ShapeDtypeStruct((rows, LANES), BF16)
    vmem = pl.BlockSpec(memory_space=pltpu.VMEM)
    return pl.pallas_call(
        token_kernel,
        in_specs=[pl.BlockSpec(memory_space=pltpu.SMEM)]
        + [vmem] * 9
        + [pl.BlockSpec(memory_space=pltpu.HBM)],
        out_specs=[vmem] * 6,
        out_shape=[half] * 4
        + [jax.ShapeDtypeStruct((rows, LANES), F32), jax.ShapeDtypeStruct((2, rows), F32)],
        scratch_shapes=[
            pltpu.VMEM((rows, weights.shape[0]), BF16),
            pltpu.VMEM((LANES, rows), F32),
            pltpu.VMEM((FACETS, rows), F32),
            pltpu.SemaphoreType.DMA,
        ],
        compiler_params=pltpu.CompilerParams(vmem_limit_bytes=20 << 20),
        name="token_projection",
    )(bias, *pieces, weights, in_hbm(decay.T))


def cell_kernel(q_ref, k_ref, v_ref, gate_ref, facet_ref, out_ref):
    row = lax.broadcasted_iota(jnp.int32, (SEG, SEG), 0)
    col = lax.broadcasted_iota(jnp.int32, (SEG, SEG), 1)
    causal = row >= col
    eye = row == col
    scale = LANES ** (-0.5)

    def to_row(column):
        return jnp.sum(jnp.where(eye, column, 0.0), axis=0, keepdims=True)

    def to_col(line):
        return jnp.sum(jnp.where(eye, line, 0.0), axis=1, keepdims=True)

    memory = jnp.zeros((LANES, LANES), F32)
    normal = jnp.zeros((1, LANES), F32)
    stabilizer = jnp.full((1, 1), EMPTY_LOG, F32)
    for b in range(q_ref.shape[0] // SEG):
        part = slice(b * SEG, (b + 1) * SEG)
        q = q_ref[part, :]
        k = k_ref[part, :]
        v = v_ref[part, :]
        in_row = gate_ref[0:1, part]
        cum_col = jnp.sum(jnp.where(causal, gate_ref[1:2, part], 0.0), axis=1, keepdims=True)
        cum_row = to_row(cum_col)
        log_weight = jnp.where(causal, cum_col - cum_row + in_row, -jnp.inf)
        carried = cum_col + stabilizer
        peak = jnp.maximum(carried, jnp.max(log_weight, axis=1, keepdims=True))
        weight = jnp.exp(log_weight - peak)
        old = jnp.exp(carried - peak)
        logits = dot(q, k, ((1,), (1,))) * scale * weight
        high, low = split_bf16(logits)
        mem_high, mem_low = split_bf16(memory)
        numerator = old * (dot(q, mem_high) + dot(q, mem_low)) + (dot(high, v) + dot(low, v))
        denominator = old * jnp.sum(q.astype(F32) * normal, axis=1, keepdims=True) + jnp.sum(
            logits, axis=1, keepdims=True
        )
        cell = numerator / jnp.maximum(jnp.abs(denominator), jnp.exp(-peak))
        square = jnp.mean(cell * cell, axis=1, keepdims=True)
        out_ref[part, :] = cell * lax.rsqrt(square + EPS) * facet_ref[...]
        peak_last = peak[SEG - 1 :, :]
        cum_last = cum_col[SEG - 1 :, :]
        old_last = old[SEG - 1 :, :]
        last = jnp.exp(to_col(cum_last - cum_row + in_row) - peak_last)
        weighted = k.astype(F32) * scale * last
        wk_high, wk_low = split_bf16(weighted)
        memory = old_last * memory + (
            dot(wk_high, v, ((0,), (0,))) + dot(wk_low, v, ((0,), (0,)))
        )
        normal = old_last * normal + jnp.sum(weighted, axis=0, keepdims=True)
        stabilizer = peak_last


def cell_block(q, k, v, gates, facet):
    vmem = pl.BlockSpec(memory_space=pltpu.VMEM)
    return pl.pallas_call(
        cell_kernel,
        in_specs=[vmem] * 5,
        out_specs=vmem,
        out_shape=jax.ShapeDtypeStruct(q.shape, F32),
        compiler_params=pltpu.CompilerParams(vmem_limit_bytes=8 << 20),
        name="cell",
    )(q, k, v, gates, facet.reshape(1, LANES))


def passage(halves, at):
    first, second = (ref[low(at, ref.shape[0])] for ref in halves)
    return jnp.where(at < halves[0].shape[0], first, second)


def select_kernel(deltas, plan_ref, *refs):
    arrays, outs = refs[: 2 * len(deltas)], refs[2 * len(deltas) :]
    for p, delta in enumerate(deltas):
        for turn in range(NX):
            for slot in range(2):
                at = plan_ref[turn, delta * 2 + slot]
                outs[turn][p, slot] = passage(arrays[2 * p : 2 * p + 2], at)


def far_kernel(plan_ref, *refs):
    arrays, outs = refs[:4], refs[4:]
    for turn in range(NX):
        way = turn // 2
        for slot in range(2):
            at = plan_ref[turn, way * 2 + slot]
            outs[turn][slot] = passage(arrays[way * 2 : way * 2 + 2], at)


def pick(kernel, plan, arrays, planes):
    vmem = pl.BlockSpec(memory_space=pltpu.VMEM)
    out = jax.ShapeDtypeStruct(planes + (2,) + arrays[0].shape[1:], BF16)
    return pl.pallas_call(
        kernel,
        in_specs=[pl.BlockSpec(memory_space=pltpu.SMEM)] + [vmem] * len(arrays),
        out_specs=[vmem] * NX,
        out_shape=[out] * NX,
        compiler_params=pltpu.CompilerParams(vmem_limit_bytes=8 << 20),
    )(plan, *arrays)


def select(plan, held):
    deltas = [delta for delta, _, _ in held]
    arrays = [a for _, first, second in held for a in (first, second)]
    kernel = functools.partial(select_kernel, deltas)
    return deltas, pick(kernel, plan, arrays, (len(deltas),))


def read_kernel(groups, plan_ref, scale_ref, *refs):
    across = refs[: len(groups) * NX]
    far = refs[len(groups) * NX : (len(groups) + 1) * NX]
    ask_ref, mix_ref, cell_ref, out_ref, kv_scr, k_scr, v_scr = refs[(len(groups) + 1) * NX :]
    for n, deltas in enumerate(groups):
        for turn in range(NX):
            for p, delta in enumerate(deltas):
                kv_scr[delta, turn] = across[n * NX + turn][p]
    for turn in range(NX):
        kv_scr[NZ // 2, turn] = far[turn][...]
    row = lax.broadcasted_iota(jnp.int32, (SEG, SEG), 0)
    col = lax.broadcasted_iota(jnp.int32, (SEG, SEG), 1)
    eye = row == col
    length = k_scr.shape[0] // 4
    score_scale = scale_ref[lax.axis_index("tp")] / LANES
    blocks = out_ref.shape[0] // SEG
    for b in range(blocks):
        part = slice(b * SEG, (b + 1) * SEG)
        for i in range(4):
            place = plan_ref[0, PLACE_AT + i * blocks + b]
            delta = shift(place, NX * 2)
            turn = low(shift(place, 2), NX)
            slot = low(place, 2)
            rows = slice(i * length, (i + 1) * length)
            k_scr[rows, :] = kv_scr[delta, turn, slot, 0]
            v_scr[rows, :] = kv_scr[delta, turn, slot, 1]
        ask = ask_ref[part, :]
        keys = k_scr[...]
        ask32 = ask.astype(F32)
        key32 = keys.astype(F32)
        ask_scale = lax.rsqrt(jnp.mean(ask32 * ask32, axis=1, keepdims=True) + EPS)
        ask_row = jnp.sum(jnp.where(eye, ask_scale, 0.0), axis=0, keepdims=True)
        key_scale = lax.rsqrt(jnp.mean(key32 * key32, axis=1, keepdims=True) + EPS)
        scores = dot(keys, ask, ((1,), (1,))) * ask_row * key_scale * score_scale
        peak = jnp.max(scores, axis=0, keepdims=True)
        terms = jnp.exp(scores - peak)
        weights = (terms / jnp.sum(terms, axis=0, keepdims=True)).astype(BF16)
        retrieved = dot(weights, v_scr[...], ((0,), (0,)))
        gate = 1.0 / (1.0 + jnp.exp(-mix_ref[part, :]))
        out_ref[part, :] = (cell_ref[part, :] + gate * retrieved).astype(BF16)


def read_passages(plan, scale, stages, far, ask, mix, cell):
    groups = [d for d, _ in stages]
    arrays = [a for _, turned in stages for a in turned] + far
    length, lanes = arrays[0].shape[-2:]
    vmem = pl.BlockSpec(memory_space=pltpu.VMEM)
    smem = pl.BlockSpec(memory_space=pltpu.SMEM)
    hbm = pl.BlockSpec(memory_space=pltpu.HBM)
    return pl.pallas_call(
        functools.partial(read_kernel, groups),
        in_specs=[smem, smem] + [vmem] * (len(arrays) + 3),
        out_specs=vmem,
        out_shape=jax.ShapeDtypeStruct(ask.shape, BF16),
        scratch_shapes=[
            pltpu.VMEM((NZ, NX, 2, 2, length, lanes), BF16),
            pltpu.VMEM((4 * length, lanes), BF16),
            pltpu.VMEM((4 * length, lanes), BF16),
        ],
        compiler_params=pltpu.CompilerParams(vmem_limit_bytes=16 << 20),
        name="read_passages",
    )(plan, scale, *arrays, ask, mix, cell)


def send(tensor, up, turn):
    pairs = [
        (z * NX + x, (z + up) % NZ * NX + (x + turn) % NX) for z in range(NZ) for x in range(NX)
    ]
    return lax.ppermute(tensor, "st", pairs)


def along_x(picked):
    return [picked[0]] + [send(picked[t], 0, t) for t in range(1, NX)]


def to_tp(tensor, step, other):
    pairs = [
        (y * 2 + c, (y + step) % 4 * 2 + (1 - c if other else c)) for y in range(4) for c in range(2)
    ]
    return lax.ppermute(tensor, "tp", pairs)


def gather_tokens(tokens):
    own = [tokens] + [to_tp(tokens, d, False) for d in (1, -1, 2)]
    return own + [to_tp(p, 0, True) for p in own]


def body(
    symbol_activations,
    document_corpus,
    document_choice_matrix,
    memory_probe_matrix,
    memory_lookup_matrix,
    memory_content_matrix,
    valve_matrix,
    valve_biases,
    added_decay_logit,
    facet_rescale_factor,
    document_probe_matrix,
    document_lookup_matrix,
    document_content_matrix,
    document_rescale_factor,
    affinity_scaling,
    fetched_mixer_matrix,
):
    per_owner = document_corpus.shape[0]
    ids = document_choice_matrix.T

    own, joined = passage_projection(
        document_corpus,
        document_rescale_factor,
        document_lookup_matrix,
        document_content_matrix,
        [
            memory_probe_matrix,
            memory_lookup_matrix,
            memory_content_matrix,
            document_probe_matrix,
            fetched_mixer_matrix,
        ],
        valve_matrix,
    )
    pieces = gather_tokens(symbol_activations)
    readers = [ids] + [send(ids, 0, -turn) for turn in range(1, NX)]
    kernel = functools.partial(plan_kernel, per_owner)
    plan, plane_ids = plan_call(kernel, readers, 2)
    near = (send(plane_ids, -1, 0), send(plane_ids, 1, 0))
    kernel = functools.partial(far_plan_kernel, per_owner, ids.size)
    (far_plan,) = plan_call(kernel, near, 1)

    up, down = list(own), list(own)
    held = [(0, *own)]
    stages = []
    for step in range(1, 4):
        for n in range(2):
            up[n] = in_vmem(send(up[n], 1, 0))
            down[n] = in_vmem(send(down[n], -1, 0))
        held += [(NZ - step, *up), (step, *down)]
        deltas, picked = select(plan, held)
        held = []
        stages.append((deltas, along_x(picked)))
    far = pick(far_kernel, far_plan, [*up, *down], ())
    far = [send(far[t], 1 if t < 2 else -1, t) for t in range(NX)]

    q, k, v, ask, mix, gates = token_projection(pieces, joined, valve_biases, added_decay_logit)
    cell = cell_block(q, k, v, gates, facet_rescale_factor)
    return read_passages(plan, affinity_scaling, stages, far, ask, mix, cell)


def solution(mesh):
    return jax.shard_map(
        body,
        mesh=mesh,
        in_specs=(
            P("st", "tp"),
            P("st", None, None),
            P("st", None),
            P(None, "tp"),
            P(None, "tp"),
            P(None, "tp"),
            P(),
            P(),
            P("st", None),
            P("tp"),
            P(None, "tp"),
            P(None, "tp"),
            P(None, "tp"),
            P(),
            P(),
            P(None, "tp"),
        ),
        out_specs=P("st", "tp"),
        check_vma=False,
    )
```
